512 devices in a mesh: sp: 128 (over z, x, core), tp: 4 (over y).
Axes of the slice: x: 4, y: 4, z: 16, core: 2. Of those that a mesh axis runs over, the one named last changes fastest.
Arguments:
- tokens: bfloat16 [65536, 2048], P('sp', 'tp'), may hold values from -6 to 6
- norm_gain: float32 [2048], replicated, may hold values from 0.1 to 1.9
- w_query: bfloat16 [2048, 1024], P('sp', 'tp'), may hold values from -1 to 1
- w_key: bfloat16 [2048, 256], P('sp', 'tp'), may hold values from -16 to 16
- w_value: bfloat16 [2048, 256], P('sp', 'tp'), may hold values from -1 to 1
- w_post_gate: bfloat16 [2048, 1024], P('sp', 'tp'), may hold values from -0.125 to 0.125
- w_pre_gate: bfloat16 [2048, 1024], P('sp', 'tp'), may hold values from -0.125 to 0.125
- w_conv_in: bfloat16 [2048, 1024], P('sp', 'tp'), may hold values from -0.125 to 0.125
- conv_taps: float32 [3, 1024], P(None, 'tp'), may hold values from -3 to 3
- sink_logit: float32 [16], P('tp'), may hold values from 2 to 6
- w_out_attn: bfloat16 [1024, 2048], P('tp', 'sp'), may hold values from -0.1875 to 0.1875
- w_out_conv: bfloat16 [1024, 2048], P('tp', 'sp'), may hold values from -0.1875 to 0.1875
Outputs:
- mixed: bfloat16 [65536, 2048], P(('sp', 'tp'))
- log_weight_sum: float32 [16, 65536], P('tp', 'sp')
The draws below stay inside these ranges and needn't reach their ends.
All inputs are finite; a program needn't handle non-finite values.
Results may differ from the reference program's by a relative error of at most 0.012.
The reference program's roundings to bfloat16 on the way count: a program that leaves them out, or rounds other values in their place, can miss the bound.
Values may be sent and summed in bfloat16 or wider, within the bound.
No kernel may reach another device: no remote copies, remote signals or barrier semaphores. Data moves between devices by JAX's collectives and lax.ppermute only.
A program may use at most 64 MiB of HBM per device.

```python
import jax
import jax.numpy as jnp
from jax import lax

D = 2048
HEADS = 16
KV_HEADS = 4
HEAD_DIM = 64
CONV_CH = 1024
WINDOW = 128
GRID_W = 64
TOKENS = 65536


def query_key_pair(key):
    base = jax.random.fold_in(key, 11)
    query_seed, key_seed = jax.random.split(base, 2)
    fan_scale = D ** (-0.5)
    w_query = jnp.clip(jax.random.normal(query_seed, (D, HEADS * HEAD_DIM), jnp.float32), -6.0, 6.0) * fan_scale
    w_key = jnp.clip(jax.random.normal(key_seed, (D, KV_HEADS * HEAD_DIM), jnp.float32), -6.0, 6.0) * fan_scale
    return (w_query, w_key)


def draw_w_query(key, part):
    return query_key_pair(key)[0].astype(jnp.bfloat16)


def draw_w_key(key, part):
    return query_key_pair(key)[1].astype(jnp.bfloat16)


def steps_of(stream_key, dims, shards, smallest, high):
    factor_of, own = 1.0, jax.random.fold_in(stream_key, 6)
    for axis_at, blocks in shards:
        draws = jnp.exp(jax.random.uniform(jax.random.fold_in(own, axis_at), (blocks,), jnp.float32, smallest / len(shards), high / len(shards)))
        factor_of = factor_of * jnp.repeat(draws, dims[axis_at] // blocks).reshape([-1 if axis == axis_at else 1 for axis in range(len(dims))])
    return factor_of


def normal_values(key, dims, spread, limit, shards=(), kind=jnp.bfloat16):
    array = jax.random.normal(key, dims, jnp.float32) * spread
    if len(shards) > 0:
        array = steps_of(key, dims, shards, -0.22, 0.18) * array
    return jnp.clip(array, min=-limit, max=limit).astype(kind)


def setup_inputs(seed: int = 0) -> dict:
    streams_of = jax.random.split(jax.random.key(seed), 13)
    return {
        "tokens": normal_values(streams_of[0], (TOKENS, D), 1.0, 6.0, ((0, 128), (1, 4))),
        "norm_gain": jnp.clip(1.0 + 0.18 * jax.random.normal(streams_of[1], (D,), jnp.float32), 0.1, 1.9),
        "w_query": draw_w_query(jax.random.fold_in(streams_of[12], 71), 0),
        "w_key": draw_w_key(jax.random.fold_in(streams_of[12], 71), 0),
        "w_value": normal_values(streams_of[4], (D, KV_HEADS * HEAD_DIM), (D // 64) ** -0.5, 1.0, ((0, 128), (1, 4))),
        "w_post_gate": normal_values(streams_of[5], (D, CONV_CH), D ** -0.5, 0.125, ((0, 128), (1, 4))),
        "w_pre_gate": normal_values(streams_of[6], (D, CONV_CH), D ** -0.5, 0.125, ((0, 128), (1, 4))),
        "w_conv_in": normal_values(streams_of[7], (D, CONV_CH), D ** -0.5, 0.125, ((0, 128), (1, 4))),
        "conv_taps": normal_values(streams_of[8], (3, CONV_CH), 0.6, 3.0, ((1, 4),), jnp.float32),
        "sink_logit": jnp.clip(2.0 + 4.0 * jax.random.uniform(streams_of[9], (HEADS,), jnp.float32) ** steps_of(streams_of[9], (HEADS,), ((0, 4),), -0.2, 0.2), 2.0, 6.0),
        "w_out_attn": normal_values(streams_of[10], (HEADS * HEAD_DIM, D), (HEADS * HEAD_DIM) ** -0.5, 0.1875, ((0, 4), (1, 128))),
        "w_out_conv": normal_values(streams_of[11], (CONV_CH, D), CONV_CH ** -0.5, 0.1875, ((0, 4), (1, 128))),
    }


rope_base = 10000.0
norm_eps = 1e-06

def rotate_pair(values, angles):
    first_half, second_half = jnp.split(values, 2, axis=-1)
    cosine = jnp.cos(angles)[:, None, :]
    sine_part = jnp.sin(angles)[:, None, :]
    return jnp.concatenate([first_half * cosine - second_half * sine_part, first_half * sine_part + second_half * cosine], axis=-1)

def axial_rotate(values, positions):
    half_dim = values.shape[-1] // 2
    inv_freq = rope_base ** (-jnp.arange(0, half_dim, 2).astype(jnp.float32) / half_dim)
    row_angle = (positions // GRID_W).astype(jnp.float32)[:, None] * inv_freq
    col_angle = (positions % GRID_W).astype(jnp.float32)[:, None] * inv_freq
    row_part, col_part = jnp.split(values, 2, axis=-1)
    return jnp.concatenate([rotate_pair(row_part, row_angle), rotate_pair(col_part, col_angle)], axis=-1)

def reference(tokens, norm_gain, w_query, w_key, w_value, w_post_gate, w_pre_gate, w_conv_in, conv_taps, sink_logit, w_out_attn, w_out_conv):
    total_tokens = tokens.shape[0]
    whole = tokens.astype(jnp.float32)
    normed = (whole * lax.rsqrt(lax.optimization_barrier(jnp.mean(whole * whole, axis=1, keepdims=True)) + norm_eps) * norm_gain.astype(jnp.float32)).astype(jnp.bfloat16)

    def project(weight):
        return jnp.dot(normed, weight, preferred_element_type=jnp.float32)
    positions = jnp.arange(total_tokens, dtype=jnp.int32)
    queries = axial_rotate(project(w_query).reshape(total_tokens, HEADS, HEAD_DIM), positions).astype(jnp.bfloat16)
    keys_rot = axial_rotate(project(w_key).reshape(total_tokens, KV_HEADS, HEAD_DIM), positions).astype(jnp.bfloat16)
    values_all = project(w_value).astype(jnp.bfloat16).reshape(total_tokens, KV_HEADS, HEAD_DIM)
    mixed_input = lax.optimization_barrier((project(w_pre_gate) * project(w_conv_in)).astype(jnp.bfloat16)).astype(jnp.float32)
    padded = jnp.pad(mixed_input, ((1, 1), (0, 0)))
    tap_weights = conv_taps.astype(jnp.float32)
    convolved = tap_weights[0] * padded[:-2] + tap_weights[1] * padded[1:-1] + tap_weights[2] * padded[2:]
    conv_out = (project(w_post_gate) * convolved).astype(jnp.bfloat16)
    blocks = total_tokens // WINDOW
    group_size = HEADS // KV_HEADS
    pad_spec = ((WINDOW, WINDOW), (0, 0), (0, 0))
    keys_pad = jnp.pad(keys_rot, pad_spec)
    values_pad = jnp.pad(values_all, pad_spec)
    block_queries = queries.reshape(blocks, WINDOW, KV_HEADS, group_size, HEAD_DIM)
    sink_values = sink_logit.astype(jnp.float32).reshape(KV_HEADS, group_size)[:, :, None]

    def one_block(inputs):
        query_block, index = inputs
        key_block = lax.dynamic_slice_in_dim(keys_pad, index * WINDOW, 3 * WINDOW, 0)
        value_block = lax.dynamic_slice_in_dim(values_pad, index * WINDOW, 3 * WINDOW, 0)
        scores = jnp.einsum('qkgd,skd->kgqs', query_block.astype(jnp.float32), key_block.astype(jnp.float32)) * HEAD_DIM ** (-0.5)
        query_pos = index * WINDOW + jnp.arange(WINDOW, dtype=jnp.int32)
        key_pos = index * WINDOW - WINDOW + jnp.arange(3 * WINDOW, dtype=jnp.int32)
        allowed = (jnp.abs(key_pos[None, :] - query_pos[:, None]) <= WINDOW) & (key_pos >= 0)[None, :] & (key_pos < total_tokens)[None, :]
        scores = jnp.where(allowed[None, None], scores, -jnp.inf)
        row_max = jnp.maximum(lax.optimization_barrier(jnp.max(scores, axis=-1)), sink_values)
        exp_scores = jnp.exp(scores - row_max[..., None])
        denominator = lax.optimization_barrier(jnp.sum(exp_scores, axis=-1)) + jnp.exp(sink_values - row_max)
        weights = (exp_scores / denominator[..., None]).astype(jnp.bfloat16)
        attended = jnp.einsum('kgqs,skd->qkgd', weights.astype(jnp.float32), value_block.astype(jnp.float32)).astype(jnp.bfloat16)
        return (attended.reshape(WINDOW, HEADS * HEAD_DIM), row_max + jnp.log(denominator))
    attended, log_sum = lax.map(one_block, (block_queries, jnp.arange(blocks, dtype=jnp.int32)))
    attended = attended.reshape(total_tokens, HEADS * HEAD_DIM)
    log_weight_sum = jnp.transpose(log_sum, (1, 2, 0, 3)).reshape(HEADS, total_tokens)
    mixed = (jnp.dot(attended, w_out_attn, preferred_element_type=jnp.float32) + jnp.dot(conv_out, w_out_conv, preferred_element_type=jnp.float32)).astype(jnp.bfloat16)
    return (mixed, log_weight_sum)
```

```python
import jax
import jax.numpy as jnp
from jax import lax
from jax.experimental import pallas as pl
from jax.experimental.pallas import tpu as pltpu
from jax.sharding import Mesh
from jax.sharding import PartitionSpec as P

HEAD_DIM = 64
WINDOW = 128
GRID_W = 64
SP = ("sp_0", "sp_1", "sp_2")
SP_TP = ("sp_0", "sp_1", "sp_2", "tp")


rope_base = 10000.0
norm_eps = 1e-06


Z, X, CORE = "sp_0", "sp_1", "sp_2"
SLOTS = (0, 4, 8, 12, 1, 5, 9, 13, 15, 3, 7, 11, 2, 6, 14, 10)


def from_offset(x, axis, offset):
    count = lax.axis_size(axis)
    return lax.ppermute(x, axis, [((i + offset) % count, i) for i in range(count)])


def gathered_z(piece):
    quarter = jnp.stack([piece] + [from_offset(piece, Z, step) for step in (4, 8, -4)])
    up = from_offset(quarter, Z, 1)
    down = from_offset(quarter, Z, -1)
    up_2 = from_offset(quarter[:2], Z, 2)
    down_2 = from_offset(jnp.stack([quarter[0], quarter[3]]), Z, -2)
    return jnp.concatenate([quarter, up, down, up_2, down_2])


def gathered_in(piece):
    own = gathered_z(piece)
    up = from_offset(own, X, 1)
    down = from_offset(own, X, -1)
    far_a = from_offset(up[:8], X, 1)
    far_b = from_offset(down[8:], X, -1)
    mine = (own, up, far_a, far_b, down)
    return mine, tuple(from_offset(part, CORE, 1) for part in mine)


def assemble_in_kernel(*refs):
    *parts, out_ref = refs
    z, x, core = lax.axis_index(Z), lax.axis_index(X), lax.axis_index(CORE)
    for side in range(2):
        for k, (x_rel, first) in enumerate(((0, 0), (1, 0), (2, 0), (2, 8), (3, 0))):
            ref = parts[5 * side + k]
            for slot in range(ref.shape[0]):
                row = lax.rem(z + SLOTS[first + slot], 16) * 4 + lax.rem(x + x_rel, 4)
                row = row * 2 + lax.rem(core + side, 2)
                out_ref[pl.ds(pl.multiple_of(row * 16, 16), 16), :] = ref[slot]


def assemble_out_kernel(mine_ref, other_ref, out_ref):
    x, core = lax.axis_index(X), lax.axis_index(CORE)
    for side, ref in enumerate((mine_ref, other_ref)):
        for z in range(16):
            for x_rel in range(4):
                row = (z * 4 + lax.rem(x + x_rel, 4)) * 2 + lax.rem(core + side, 2)
                out_ref[pl.ds(pl.multiple_of(row * 16, 16), 16), :] = ref[z, x_rel]


VMEM = pl.BlockSpec(memory_space=pltpu.VMEM)


def assembled_in(mine, other):
    parts = (*mine, *other)
    width = parts[0].shape[-1]
    return pl.pallas_call(
        assemble_in_kernel,
        out_shape=jax.ShapeDtypeStruct((2048, width), jnp.bfloat16),
        in_specs=[VMEM] * len(parts),
        out_specs=VMEM,
        cost_estimate=pl.CostEstimate(flops=2_000_000, bytes_accessed=9_000_000, transcendentals=0),
    )(*parts)


def gathered_out(piece):
    stack = jnp.stack([piece] + [from_offset(piece, X, step) for step in (1, 2, 3)])
    own = lax.all_gather(stack, Z, axis=0)
    other = from_offset(own, CORE, 1)
    return pl.pallas_call(
        assemble_out_kernel,
        out_shape=jax.ShapeDtypeStruct((2048, piece.shape[-1]), jnp.bfloat16),
        in_specs=[VMEM] * 2,
        out_specs=VMEM,
        cost_estimate=pl.CostEstimate(flops=2_000_000, bytes_accessed=4_000_000, transcendentals=0),
    )(own, other)


def gathered_tokens(tokens):
    tp = lax.axis_index("tp")
    parts = [tokens] + [from_offset(tokens, "tp", step) for step in (1, 2, 3)]
    rows, width = tokens.shape
    whole = jnp.zeros((rows, 4 * width), tokens.dtype)
    for step, part in enumerate(parts):
        whole = lax.dynamic_update_slice(whole, part, (0, lax.rem(tp + step, 4) * width))
    return whole


def summed_at_owner(x):
    tp = lax.axis_index("tp")
    rows = x.shape[0] // 4
    total = lax.dynamic_slice_in_dim(x, tp * rows, rows, 0).astype(jnp.float32)
    for step in (1, 2, 3):
        block = lax.dynamic_slice_in_dim(x, lax.rem(tp + step, 4) * rows, rows, 0)
        total = total + from_offset(block, "tp", -step).astype(jnp.float32)
    return total


def padded_halo(block, width):
    count = lax.axis_size(SP)
    forward = [(i, i + 1) for i in range(count - 1)]
    backward = [(i + 1, i) for i in range(count - 1)]
    low = lax.ppermute(block[-width:], SP, forward)
    high = lax.ppermute(block[:width], SP, backward)
    return jnp.concatenate([low, block, high], axis=0)


def rotate_pair(values, angles):
    first_half, second_half = jnp.split(values, 2, axis=-1)
    cosine = jnp.cos(angles)[:, None, :]
    sine_part = jnp.sin(angles)[:, None, :]
    return jnp.concatenate(
        [
            first_half * cosine - second_half * sine_part,
            first_half * sine_part + second_half * cosine,
        ],
        axis=-1,
    )


def axial_rotate(values, positions):
    half_dim = values.shape[-1] // 2
    inv_freq = rope_base ** (-jnp.arange(0, half_dim, 2).astype(jnp.float32) / half_dim)
    row_angle = (positions // GRID_W).astype(jnp.float32)[:, None] * inv_freq
    col_angle = (positions % GRID_W).astype(jnp.float32)[:, None] * inv_freq
    row_part, col_part = jnp.split(values, 2, axis=-1)
    return jnp.concatenate(
        [rotate_pair(row_part, row_angle), rotate_pair(col_part, col_angle)], axis=-1
    )


def block_windows(source, rows_local, blocks):
    pieces = [
        source[step * WINDOW : step * WINDOW + rows_local].reshape(
            (blocks, WINDOW) + source.shape[1:]
        )
        for step in range(3)
    ]
    return jnp.concatenate(pieces, axis=1)


def on_device(
    tokens,
    norm_gain,
    w_query,
    w_key,
    w_value,
    w_post_gate,
    w_pre_gate,
    w_conv_in,
    conv_taps,
    sink_logit,
    w_out_attn,
    w_out_conv,
):
    whole = gathered_tokens(tokens)
    rows_local = whole.shape[0]
    whole_float = whole.astype(jnp.float32)
    mean_square = jnp.mean(whole_float * whole_float, axis=1, keepdims=True)
    normed = (whole_float * lax.rsqrt(mean_square + norm_eps) * norm_gain).astype(jnp.bfloat16)
    col_widths = [
        w_query.shape[1],
        w_key.shape[1],
        w_value.shape[1],
        w_post_gate.shape[1],
        w_pre_gate.shape[1],
        w_conv_in.shape[1],
    ]
    piece = jnp.concatenate(
        [w_query, w_key, w_value, w_post_gate, w_pre_gate, w_conv_in], axis=1
    )
    out_piece = jnp.concatenate([w_out_attn.T, w_out_conv.T], axis=1)
    out_rows = gathered_out(out_piece)
    joined = assembled_in(*gathered_in(piece))
    projected = jnp.dot(normed, joined, preferred_element_type=jnp.float32)
    bounds = []
    running = 0
    for col_width in col_widths[:-1]:
        running += col_width
        bounds.append(running)
    query_raw, key_raw, value_raw, post_gate, pre_gate, conv_input = jnp.split(
        projected, bounds, axis=1
    )
    offset = lax.axis_index(SP) * rows_local
    positions = offset + jnp.arange(rows_local, dtype=jnp.int32)
    local_heads = w_query.shape[1] // HEAD_DIM
    local_groups = w_key.shape[1] // HEAD_DIM
    group_size = local_heads // local_groups
    queries = axial_rotate(query_raw.reshape(rows_local, local_heads, HEAD_DIM), positions).astype(
        jnp.bfloat16
    )
    keys_rot = axial_rotate(key_raw.reshape(rows_local, local_groups, HEAD_DIM), positions).astype(
        jnp.bfloat16
    )
    key_value = jnp.concatenate(
        [keys_rot.reshape(rows_local, local_groups * HEAD_DIM), value_raw.astype(jnp.bfloat16)],
        axis=1,
    )
    mixed_input = (pre_gate * conv_input).astype(jnp.bfloat16)
    kv_width = key_value.shape[1]
    padded = padded_halo(jnp.concatenate([key_value, mixed_input], axis=1), WINDOW)
    kv_padded = padded[:, :kv_width]
    conv_padded = padded[WINDOW - 1 : WINDOW + rows_local + 1, kv_width:]
    conv_float = conv_padded.astype(jnp.float32)
    convolved = (
        conv_taps[0] * conv_float[:-2]
        + conv_taps[1] * conv_float[1:-1]
        + conv_taps[2] * conv_float[2:]
    )
    conv_out = (post_gate * convolved).astype(jnp.bfloat16)
    total_tokens = rows_local * lax.axis_size(SP)
    blocks = rows_local // WINDOW
    padded_rows = rows_local + 2 * WINDOW
    block_queries = queries.reshape(blocks, WINDOW, local_groups, group_size, HEAD_DIM)
    block_keys = block_windows(
        kv_padded[:, : local_groups * HEAD_DIM].reshape(padded_rows, local_groups, HEAD_DIM),
        rows_local,
        blocks,
    )
    block_values = block_windows(
        kv_padded[:, local_groups * HEAD_DIM :].reshape(padded_rows, local_groups, HEAD_DIM),
        rows_local,
        blocks,
    )
    scores = jnp.einsum(
        "nqkgd,nskd->nkgqs", block_queries, block_keys, preferred_element_type=jnp.float32
    ) * HEAD_DIM ** (-0.5)
    query_pos = positions.reshape(blocks, WINDOW)
    key_pos = (
        offset
        - WINDOW
        + (jnp.arange(blocks, dtype=jnp.int32) * WINDOW)[:, None]
        + jnp.arange(3 * WINDOW, dtype=jnp.int32)[None, :]
    )
    distance = key_pos[:, None, :] - query_pos[:, :, None]
    allowed = (
        (jnp.abs(distance) <= WINDOW)
        & (key_pos >= 0)[:, None, :]
        & (key_pos < total_tokens)[:, None, :]
    )
    scores = jnp.where(allowed[:, None, None], scores, -jnp.inf)
    sink_values = sink_logit.reshape(local_groups, group_size)[None, :, :, None]
    row_max = jnp.maximum(jnp.max(scores, axis=-1), sink_values)
    exp_scores = jnp.exp(scores - row_max[..., None])
    denominator = jnp.sum(exp_scores, axis=-1) + jnp.exp(sink_values - row_max)
    weights = (exp_scores / denominator[..., None]).astype(jnp.bfloat16)
    attended = (
        jnp.einsum("nkgqs,nskd->nqkgd", weights, block_values, preferred_element_type=jnp.float32)
        .astype(jnp.bfloat16)
        .reshape(rows_local, local_heads * HEAD_DIM)
    )
    log_sum = row_max + jnp.log(denominator)
    log_weight_sum = jnp.transpose(log_sum, (1, 2, 0, 3)).reshape(local_heads, rows_local)
    both = jnp.concatenate([attended, conv_out], axis=1)
    partial = lax.dot_general(
        both, out_rows, (((1,), (1,)), ((), ())), preferred_element_type=jnp.float32
    ).astype(jnp.bfloat16)
    mixed = summed_at_owner(partial).astype(jnp.bfloat16)
    return (mixed, log_weight_sum)


def solution(mesh):
    torus = Mesh(mesh.devices.reshape(16, 4, 2, mesh.shape["tp"]), ("sp_0", "sp_1", "sp_2", "tp"))
    return jax.shard_map(
        on_device,
        mesh=torus,
        in_specs=(
            P(SP, "tp"),
            P(),
            P(SP, "tp"),
            P(SP, "tp"),
            P(SP, "tp"),
            P(SP, "tp"),
            P(SP, "tp"),
            P(SP, "tp"),
            P(None, "tp"),
            P("tp"),
            P("tp", SP),
            P("tp", SP),
        ),
        out_specs=(P(SP_TP, None), P("tp", SP)),
        check_vma=False,
    )
```

```python
import jax
import jax.numpy as jnp
from jax import lax
from jax.experimental import pallas as pl
from jax.experimental.pallas import tpu as pltpu
from jax.sharding import Mesh
from jax.sharding import PartitionSpec as P

HEAD_DIM = 64
WINDOW = 128
GRID_W = 64
TOKENS = 65536
SP = ("sp_0", "sp_1", "sp_2")
SP_TP = ("sp_0", "sp_1", "sp_2", "tp")


rope_base = 10000.0
norm_eps = 1e-06


Z, X, CORE = "sp_0", "sp_1", "sp_2"
SLOTS = (0, 4, 8, 12, 1, 5, 9, 13, 15, 3, 7, 11, 2, 6, 14, 10)
VMEM = pl.BlockSpec(memory_space=pltpu.VMEM)
SMEM = pl.BlockSpec(memory_space=pltpu.SMEM)
PARAMS = pltpu.CompilerParams(vmem_limit_bytes=48 * 1024 * 1024)


def from_offset(x, axis, offset):
    count = lax.axis_size(axis)
    return lax.ppermute(x, axis, [((i + offset) % count, i) for i in range(count)])


def gathered_z(piece):
    quarter = jnp.stack([piece] + [from_offset(piece, Z, step) for step in (4, 8, -4)])
    up = from_offset(quarter, Z, 1)
    down = from_offset(quarter, Z, -1)
    up_2 = from_offset(quarter[:2], Z, 2)
    down_2 = from_offset(jnp.stack([quarter[0], quarter[3]]), Z, -2)
    return jnp.concatenate([quarter, up, down, up_2, down_2])


def gathered_parts(piece):
    own = gathered_z(piece)
    up = from_offset(own, X, 1)
    down = from_offset(own, X, -1)
    far_a = from_offset(up[:8], X, 1)
    far_b = from_offset(down[8:], X, -1)
    mine = (own, up, far_a, far_b, down)
    return (*mine, *(from_offset(part, CORE, 1) for part in mine))


PART_PLACES = ((0, 0), (1, 0), (2, 0), (2, 8), (3, 0))


def rotated(x, cosine, sine):
    width = x.shape[-1]
    lane = lax.broadcasted_iota(jnp.int32, x.shape, 1)
    ahead = pltpu.roll(x, width - 16, 1)
    behind = pltpu.roll(x, 16, 1)
    return x * cosine + jnp.where(lane % 32 < 16, ahead, behind) * sine


def project_kernel(*refs):
    tokens_ref, gain_ref, cos_ref, sin_ref = refs[:4]
    parts = refs[4:14]
    kvc_ref, query_ref, post_ref, out_rows_ref = refs[14:18]
    normed_ref, rows_ref = refs[18:]
    z, x, core = lax.axis_index(Z), lax.axis_index(X), lax.axis_index(CORE)
    rows, width = tokens_ref.shape[1:]
    count = tokens_ref.shape[0]
    step_rows = 64

    def norm_step(step, carry):
        at = pl.ds(pl.multiple_of(step * step_rows, step_rows), step_rows)
        blocks = [tokens_ref[k, at, :].astype(jnp.float32) for k in range(count)]
        square = sum(jnp.sum(b * b, axis=1, keepdims=True) for b in blocks)
        scale = lax.rsqrt(square / (count * width) + norm_eps)
        for k, b in enumerate(blocks):
            cols = slice(k * width, (k + 1) * width)
            normed_ref[at, cols] = (b * scale * gain_ref[:, cols]).astype(jnp.bfloat16)
        return carry

    lax.fori_loop(0, rows // step_rows, norm_step, 0)
    in_width = rows_ref.shape[1]
    for side in range(2):
        for k, (x_rel, first) in enumerate(PART_PLACES):
            ref = parts[5 * side + k]
            for slot in range(ref.shape[0]):
                row = lax.rem(z + SLOTS[first + slot], 16) * 4 + lax.rem(x + x_rel, 4)
                row = row * 2 + lax.rem(core + side, 2)
                at = pl.ds(pl.multiple_of(row * 16, 16), 16)
                rows_ref[at, :] = ref[slot, :, :in_width]
                out_rows_ref[at, :] = ref[slot, :, in_width:]

    def projected(first, last):
        return jnp.dot(
            normed_ref[...], rows_ref[:, first:last], preferred_element_type=jnp.float32
        )

    key_value = projected(0, 128)
    lane = lax.broadcasted_iota(jnp.int32, key_value.shape, 1)
    cosine = cos_ref[...]
    sine = sin_ref[...]
    kvc_ref[:, :128] = jnp.where(
        lane < 64, rotated(key_value, cosine, sine), key_value
    ).astype(jnp.bfloat16)
    kvc_ref[:, 128:] = (projected(128, 384) * projected(384, 640)).astype(jnp.bfloat16)
    for half in range(2):
        part = projected(640 + 128 * half, 768 + 128 * half)
        query_ref[:, 128 * half : 128 * (half + 1)] = rotated(part, cosine, sine).astype(
            jnp.bfloat16
        )
    post_ref[...] = projected(896, 1152)


def project(tokens, gain, cosine, sine, parts):
    rows = tokens.shape[1]
    shapes = (
        jax.ShapeDtypeStruct((rows, 384), jnp.bfloat16),
        jax.ShapeDtypeStruct((rows, 256), jnp.bfloat16),
        jax.ShapeDtypeStruct((rows, 256), jnp.float32),
        jax.ShapeDtypeStruct((2048, 512), jnp.bfloat16),
    )
    return pl.pallas_call(
        project_kernel,
        out_shape=shapes,
        in_specs=[VMEM] * 14,
        out_specs=(VMEM,) * 4,
        scratch_shapes=[
            pltpu.VMEM((rows, 2048), jnp.bfloat16),
            pltpu.VMEM((2048, 1152), jnp.bfloat16),
        ],
        compiler_params=PARAMS,
        cost_estimate=pl.CostEstimate(
            flops=2 * rows * 2048 * 1152, bytes_accessed=14_000_000, transcendentals=0
        ),
    )(tokens, gain, cosine, sine, *parts)


def attended_block(query, keys, values, sinks, first_key, total):
    heads = query.shape[1] // HEAD_DIM
    stacked = jnp.concatenate(
        [query[:, HEAD_DIM * h : HEAD_DIM * (h + 1)] for h in range(heads)], axis=0
    )
    scores = lax.dot_general(
        stacked, keys, (((1,), (1,)), ((), ())), preferred_element_type=jnp.float32
    ) * HEAD_DIM ** (-0.5)
    row = lax.broadcasted_iota(jnp.int32, scores.shape, 0) % WINDOW
    col = lax.broadcasted_iota(jnp.int32, scores.shape, 1)
    key_pos = first_key + col
    allowed = (col >= row) & (col <= row + 2 * WINDOW) & (key_pos >= 0) & (key_pos < total)
    scores = jnp.where(allowed, scores, -jnp.inf)
    sink = jnp.concatenate([jnp.full((WINDOW, 1), s, jnp.float32) for s in sinks], axis=0)
    row_max = jnp.maximum(jnp.max(scores, axis=1, keepdims=True), sink)
    exp_scores = jnp.exp(scores - row_max)
    denominator = jnp.sum(exp_scores, axis=1, keepdims=True) + jnp.exp(sink - row_max)
    weights = (exp_scores / denominator).astype(jnp.bfloat16)
    result = jnp.dot(weights, values, preferred_element_type=jnp.float32).astype(jnp.bfloat16)
    log_sum = row_max + jnp.log(denominator)
    by_head = [slice(WINDOW * h, WINDOW * (h + 1)) for h in range(heads)]
    return (
        jnp.concatenate([result[s] for s in by_head], axis=1),
        jnp.concatenate([log_sum[s] for s in by_head], axis=1),
    )


def first_position():
    place = (lax.axis_index(Z) * 4 + lax.axis_index(X)) * 2 + lax.axis_index(CORE)
    return place * 512


def inner_kernel(sink_ref, query_ref, kvc_ref, attended_ref, log_ref):
    sinks = [sink_ref[h] for h in range(4)]
    offset = first_position()
    for n in (1, 2):
        window = slice((n - 1) * WINDOW, (n + 2) * WINDOW)
        result, log_sum = attended_block(
            query_ref[n * WINDOW : (n + 1) * WINDOW, :],
            kvc_ref[window, :HEAD_DIM],
            kvc_ref[window, HEAD_DIM : 2 * HEAD_DIM],
            sinks,
            offset + (n - 1) * WINDOW,
            TOKENS,
        )
        attended_ref[(n - 1) * WINDOW : n * WINDOW, :] = result
        log_ref[(n - 1) * WINDOW : n * WINDOW, :] = log_sum


def inner(sinks, query, kvc):
    return pl.pallas_call(
        inner_kernel,
        out_shape=(
            jax.ShapeDtypeStruct((256, 256), jnp.bfloat16),
            jax.ShapeDtypeStruct((256, 4), jnp.float32),
        ),
        in_specs=[SMEM, VMEM, VMEM],
        out_specs=(VMEM, VMEM),
        compiler_params=PARAMS,
        cost_estimate=pl.CostEstimate(
            flops=2 * 2 * 1024 * 384 * 64 * 20, bytes_accessed=2_000_000, transcendentals=400_000
        ),
    )(sinks, query, kvc)


def outer_kernel(
    sink_ref, query_ref, kvc_ref, low_ref, high_ref, post_ref, taps_ref, inner_ref, out_rows_ref,
    *refs,
):
    outs, log_ref, both_ref = refs[:4], refs[4], refs[5]
    sinks = [sink_ref[h] for h in range(4)]
    offset = first_position()
    rows = query_ref.shape[0]
    edges = (
        (0, jnp.concatenate([low_ref[:, :128], kvc_ref[: 2 * WINDOW, :128]], axis=0)),
        (3, jnp.concatenate([kvc_ref[rows - 2 * WINDOW :, :128], high_ref[:, :128]], axis=0)),
    )
    for k, (n, window) in enumerate(edges):
        result, log_sum = attended_block(
            query_ref[n * WINDOW : (n + 1) * WINDOW, :],
            window[:, :HEAD_DIM],
            window[:, HEAD_DIM:],
            sinks,
            offset + (n - 1) * WINDOW,
            TOKENS,
        )
        both_ref[n * WINDOW : (n + 1) * WINDOW, :256] = result
        log_ref[k * WINDOW : (k + 1) * WINDOW, :] = log_sum
    both_ref[WINDOW : 3 * WINDOW, :256] = inner_ref[...]
    conv = kvc_ref[:, 128:].astype(jnp.float32)
    row = lax.broadcasted_iota(jnp.int32, conv.shape, 0)
    before = low_ref[WINDOW - 16 :, 128:].astype(jnp.float32)[15:16]
    after = high_ref[:16, 128:].astype(jnp.float32)[0:1]
    previous = jnp.where(row == 0, before, pltpu.roll(conv, 1, 0))
    following = jnp.where(row == rows - 1, after, pltpu.roll(conv, rows - 1, 0))
    convolved = taps_ref[0:1] * previous + taps_ref[1:2] * conv + taps_ref[2:3] * following
    both_ref[:, 256:] = (post_ref[...] * convolved).astype(jnp.bfloat16)
    tp = lax.axis_index("tp")
    for step in (2, 1, 3, 0):
        at = pl.ds(pl.multiple_of(lax.rem(tp + step, 4) * WINDOW, WINDOW), WINDOW)
        outs[step][...] = lax.dot_general(
            both_ref[at, :],
            out_rows_ref[...],
            (((1,), (1,)), ((), ())),
            preferred_element_type=jnp.float32,
        ).astype(jnp.bfloat16)


def outer(sinks, query, kvc, low, high, post, taps, inner_attended, out_rows):
    return pl.pallas_call(
        outer_kernel,
        out_shape=(
            *([jax.ShapeDtypeStruct((128, 2048), jnp.bfloat16)] * 4),
            jax.ShapeDtypeStruct((256, 4), jnp.float32),
        ),
        in_specs=[SMEM] + [VMEM] * 8,
        out_specs=(VMEM,) * 5,
        scratch_shapes=[pltpu.VMEM((512, 512), jnp.bfloat16)],
        compiler_params=PARAMS,
        cost_estimate=pl.CostEstimate(
            flops=2 * 512 * 512 * 2048, bytes_accessed=8_000_000, transcendentals=400_000
        ),
    )(sinks, query, kvc, low, high, post, taps, inner_attended, out_rows)


def halo(block, width):
    count = lax.axis_size(SP)
    forward = [(i, i + 1) for i in range(count - 1)]
    backward = [(i + 1, i) for i in range(count - 1)]
    low = lax.ppermute(block[-width:], SP, forward)
    high = lax.ppermute(block[:width], SP, backward)
    return low, high


def rotation_tables(rows):
    positions = lax.axis_index(SP) * rows + jnp.arange(rows, dtype=jnp.int32)
    half_dim = HEAD_DIM // 2
    inv_freq = rope_base ** (-jnp.arange(0, half_dim, 2).astype(jnp.float32) / half_dim)
    row_angle = (positions // GRID_W).astype(jnp.float32)[:, None] * inv_freq
    col_angle = (positions % GRID_W).astype(jnp.float32)[:, None] * inv_freq
    angle = jnp.concatenate([row_angle, row_angle, col_angle, col_angle] * 2, axis=1)
    lane = lax.broadcasted_iota(jnp.int32, angle.shape, 1)
    sine = jnp.sin(angle)
    return jnp.cos(angle), jnp.where(lane % 32 < 16, -sine, sine)


def on_device(
    tokens,
    norm_gain,
    w_query,
    w_key,
    w_value,
    w_post_gate,
    w_pre_gate,
    w_conv_in,
    conv_taps,
    sink_logit,
    w_out_attn,
    w_out_conv,
):
    whole = lax.all_gather(tokens, "tp", axis=0)
    rows = tokens.shape[0]
    piece = jnp.concatenate(
        [
            w_key,
            w_value,
            w_pre_gate,
            w_conv_in,
            w_query,
            w_post_gate,
            w_out_attn.T,
            w_out_conv.T,
        ],
        axis=1,
    )
    parts = gathered_parts(piece)
    cosine, sine = rotation_tables(rows)
    kvc, query, post, out_rows = project(whole, norm_gain[None], cosine, sine, parts)
    low, high = halo(kvc, WINDOW)
    inner_attended, inner_log = inner(sink_logit, query, kvc)
    *outs, outer_log = outer(
        sink_logit, query, kvc, low, high, post, conv_taps, inner_attended, out_rows
    )
    arrived = [from_offset(outs[step], "tp", -step) for step in (2, 1, 3)]
    total = outs[0].astype(jnp.float32)
    for block in arrived:
        total = total + block.astype(jnp.float32)
    log_sum = jnp.concatenate([outer_log[:WINDOW], inner_log, outer_log[WINDOW:]])
    return (total.astype(jnp.bfloat16), log_sum.T)


def solution(mesh):
    torus = Mesh(mesh.devices.reshape(16, 4, 2, mesh.shape["tp"]), ("sp_0", "sp_1", "sp_2", "tp"))
    return jax.shard_map(
        on_device,
        mesh=torus,
        in_specs=(
            P(SP, "tp"),
            P(),
            P(SP, "tp"),
            P(SP, "tp"),
            P(SP, "tp"),
            P(SP, "tp"),
            P(SP, "tp"),
            P(SP, "tp"),
            P(None, "tp"),
            P("tp"),
            P("tp", SP),
            P("tp", SP),
        ),
        out_specs=(P(SP_TP, None), P("tp", SP)),
        check_vma=False,
    )
```

```python
import jax
import jax.numpy as jnp
from jax import lax
from jax.experimental import pallas as pl
from jax.experimental.pallas import tpu as pltpu
from jax.sharding import Mesh
from jax.sharding import PartitionSpec as P

HEAD_DIM = 64
WINDOW = 128
GRID_W = 64
TOKENS = 65536
SP = ("z_high", "z_low", "sp_1", "sp_2")
SP_TP = (*SP, "tp")


rope_base = 10000.0
norm_eps = 1e-06


Z, X, CORE = ("z_high", "z_low"), "sp_1", "sp_2"
VMEM = pl.BlockSpec(memory_space=pltpu.VMEM)
SMEM = pl.BlockSpec(memory_space=pltpu.SMEM)
PARAMS = pltpu.CompilerParams(vmem_limit_bytes=24 * 1024 * 1024)


def from_offset(x, axis, offset):
    count = lax.axis_size(axis)
    return lax.ppermute(x, axis, [((i + offset) % count, i) for i in range(count)])


def sent_to_all(x, axis):
    copies = jnp.broadcast_to(x, (lax.axis_size(axis), *x.shape))
    return lax.all_to_all(copies, axis, split_axis=0, concat_axis=0, tiled=True)


def after(x, other):
    return lax.optimization_barrier((x, other))[0]


def across(own):
    return (own, *(from_offset(own, X, step) for step in (1, 2, 3)))


def with_other_core(parts):
    return (*parts, *(from_offset(part, CORE, 1) for part in parts))


def norm_kernel(gain_ref, *refs):
    tokens, normed_ref = refs[:4], refs[4]
    tp = lax.axis_index("tp")
    rows, width = tokens[0].shape
    step_rows = 64

    def norm_step(step, carry):
        at = pl.ds(pl.multiple_of(step * step_rows, step_rows), step_rows)
        blocks = [ref[at, :].astype(jnp.float32) for ref in tokens]
        square = sum(jnp.sum(b * b, axis=1, keepdims=True) for b in blocks)
        scale = lax.rsqrt(square / (4 * width) + norm_eps)
        for k, b in enumerate(blocks):
            cols = pl.ds(pl.multiple_of(lax.rem(tp + k, 4) * width, width), width)
            normed_ref[at, cols] = (b * scale * gain_ref[:, cols]).astype(jnp.bfloat16)
        return carry

    lax.fori_loop(0, rows // step_rows, norm_step, 0)


def normalized(gain, tokens):
    rows, width = tokens[0].shape
    return pl.pallas_call(
        norm_kernel,
        out_shape=jax.ShapeDtypeStruct((rows, 4 * width), jnp.bfloat16),
        in_specs=[VMEM] * 5,
        out_specs=VMEM,
        compiler_params=PARAMS,
        cost_estimate=pl.CostEstimate(
            flops=500_000_000, bytes_accessed=4_000_000, transcendentals=512
        ),
    )(gain, *tokens)


def place_rows(parts, out_ref):
    x, core = lax.axis_index(X), lax.axis_index(CORE)
    for side in range(2):
        for x_rel in range(4):
            ref = parts[4 * side + x_rel]
            place = lax.rem(x + x_rel, 4) * 2 + lax.rem(core + side, 2)
            for low in range(4):
                for high in range(4):
                    row = (high * 4 + low) * 128 + place * 16
                    at = pl.ds(pl.multiple_of(row, 16), 16)
                    out_ref[at, :] = ref[low, high]


def rotated(x, cosine, sine):
    width = x.shape[-1]
    lane = lax.broadcasted_iota(jnp.int32, x.shape, 1)
    ahead = pltpu.roll(x, width - 16, 1)
    behind = pltpu.roll(x, 16, 1)
    return x * cosine + jnp.where(lane % 32 < 16, ahead, behind) * sine


def project_kernel(*refs):
    normed_ref, cos_ref, sin_ref = refs[:3]
    kvc_ref, query_ref, post_ref, rows_ref = refs[11:]
    place_rows(refs[3:11], rows_ref)

    def projected(first, last):
        return jnp.dot(
            normed_ref[...], rows_ref[:, first:last], preferred_element_type=jnp.float32
        )

    key_value = projected(0, 128)
    lane = lax.broadcasted_iota(jnp.int32, key_value.shape, 1)
    cosine = cos_ref[...]
    sine = sin_ref[...]
    kvc_ref[:, :128] = jnp.where(
        lane < 64, rotated(key_value, cosine, sine), key_value
    ).astype(jnp.bfloat16)
    kvc_ref[:, 128:] = (projected(128, 384) * projected(384, 640)).astype(jnp.bfloat16)
    for half in range(2):
        part = projected(640 + 128 * half, 768 + 128 * half)
        query_ref[:, 128 * half : 128 * (half + 1)] = rotated(part, cosine, sine).astype(
            jnp.bfloat16
        )
    post_ref[...] = projected(896, 1152)


def project(normed, cosine, sine, parts):
    rows = normed.shape[0]
    return pl.pallas_call(
        project_kernel,
        out_shape=(
            jax.ShapeDtypeStruct((rows, 384), jnp.bfloat16),
            jax.ShapeDtypeStruct((rows, 256), jnp.bfloat16),
            jax.ShapeDtypeStruct((rows, 256), jnp.float32),
        ),
        in_specs=[VMEM] * 11,
        out_specs=(VMEM,) * 3,
        scratch_shapes=[pltpu.VMEM((2048, 1152), jnp.bfloat16)],
        compiler_params=PARAMS,
        cost_estimate=pl.CostEstimate(
            flops=2 * rows * 2048 * 1152, bytes_accessed=8_000_000, transcendentals=0
        ),
    )(normed, cosine, sine, *parts)


def attended_block(query, keys, values, sinks, first_key, total):
    heads = query.shape[1] // HEAD_DIM
    stacked = jnp.concatenate(
        [query[:, HEAD_DIM * h : HEAD_DIM * (h + 1)] for h in range(heads)], axis=0
    )
    scores = lax.dot_general(
        stacked, keys, (((1,), (1,)), ((), ())), preferred_element_type=jnp.float32
    ) * HEAD_DIM ** (-0.5)
    row = lax.broadcasted_iota(jnp.int32, scores.shape, 0) % WINDOW
    col = lax.broadcasted_iota(jnp.int32, scores.shape, 1)
    key_pos = first_key + col
    allowed = (col >= row) & (col <= row + 2 * WINDOW) & (key_pos >= 0) & (key_pos < total)
    scores = jnp.where(allowed, scores, -jnp.inf)
    sink = jnp.concatenate([jnp.full((WINDOW, 1), s, jnp.float32) for s in sinks], axis=0)
    row_max = jnp.maximum(jnp.max(scores, axis=1, keepdims=True), sink)
    exp_scores = jnp.exp(scores - row_max)
    denominator = jnp.sum(exp_scores, axis=1, keepdims=True) + jnp.exp(sink - row_max)
    weights = (exp_scores / denominator).astype(jnp.bfloat16)
    result = jnp.dot(weights, values, preferred_element_type=jnp.float32).astype(jnp.bfloat16)
    log_sum = row_max + jnp.log(denominator)
    by_head = [slice(WINDOW * h, WINDOW * (h + 1)) for h in range(heads)]
    return (
        jnp.concatenate([result[s] for s in by_head], axis=1),
        jnp.concatenate([log_sum[s] for s in by_head], axis=1),
    )


def first_position():
    return lax.axis_index(SP) * 512


def inner_kernel(sink_ref, query_ref, kvc_ref, attended_ref, log_ref):
    sinks = [sink_ref[h] for h in range(4)]
    offset = first_position()
    for n in (1, 2):
        window = slice((n - 1) * WINDOW, (n + 2) * WINDOW)
        result, log_sum = attended_block(
            query_ref[n * WINDOW : (n + 1) * WINDOW, :],
            kvc_ref[window, :HEAD_DIM],
            kvc_ref[window, HEAD_DIM : 2 * HEAD_DIM],
            sinks,
            offset + (n - 1) * WINDOW,
            TOKENS,
        )
        attended_ref[(n - 1) * WINDOW : n * WINDOW, :] = result
        log_ref[(n - 1) * WINDOW : n * WINDOW, :] = log_sum


def inner(sinks, query, kvc):
    return pl.pallas_call(
        inner_kernel,
        out_shape=(
            jax.ShapeDtypeStruct((256, 256), jnp.bfloat16),
            jax.ShapeDtypeStruct((256, 4), jnp.float32),
        ),
        in_specs=[SMEM, VMEM, VMEM],
        out_specs=(VMEM, VMEM),
        compiler_params=PARAMS,
        cost_estimate=pl.CostEstimate(
            flops=2 * 2 * 1024 * 384 * 64 * 20, bytes_accessed=2_000_000, transcendentals=400_000
        ),
    )(sinks, query, kvc)


def outer_kernel(
    sink_ref, query_ref, kvc_ref, low_ref, high_ref, post_ref, taps_ref, inner_ref, mine_ref,
    other_ref, *refs,
):
    outs, log_ref, both_ref, out_rows_ref = refs[:4], refs[4], refs[5], refs[6]
    place_rows([ref.at[k] for ref in (mine_ref, other_ref) for k in range(4)], out_rows_ref)
    sinks = [sink_ref[h] for h in range(4)]
    offset = first_position()
    rows = query_ref.shape[0]
    edges = (
        (0, jnp.concatenate([low_ref[:, :128], kvc_ref[: 2 * WINDOW, :128]], axis=0)),
        (3, jnp.concatenate([kvc_ref[rows - 2 * WINDOW :, :128], high_ref[:, :128]], axis=0)),
    )
    for k, (n, window) in enumerate(edges):
        result, log_sum = attended_block(
            query_ref[n * WINDOW : (n + 1) * WINDOW, :],
            window[:, :HEAD_DIM],
            window[:, HEAD_DIM:],
            sinks,
            offset + (n - 1) * WINDOW,
            TOKENS,
        )
        both_ref[n * WINDOW : (n + 1) * WINDOW, :256] = result
        log_ref[k * WINDOW : (k + 1) * WINDOW, :] = log_sum
    both_ref[WINDOW : 3 * WINDOW, :256] = inner_ref[...]
    conv = kvc_ref[:, 128:].astype(jnp.float32)
    row = lax.broadcasted_iota(jnp.int32, conv.shape, 0)
    before = low_ref[WINDOW - 16 :, 128:].astype(jnp.float32)[15:16]
    after = high_ref[:16, 128:].astype(jnp.float32)[0:1]
    previous = jnp.where(row == 0, before, pltpu.roll(conv, 1, 0))
    following = jnp.where(row == rows - 1, after, pltpu.roll(conv, rows - 1, 0))
    convolved = taps_ref[0:1] * previous + taps_ref[1:2] * conv + taps_ref[2:3] * following
    both_ref[:, 256:] = (post_ref[...] * convolved).astype(jnp.bfloat16)
    tp = lax.axis_index("tp")
    for step in (2, 1, 3, 0):
        at = pl.ds(pl.multiple_of(lax.rem(tp + step, 4) * WINDOW, WINDOW), WINDOW)
        outs[step][...] = lax.dot_general(
            both_ref[at, :],
            out_rows_ref[...],
            (((1,), (1,)), ((), ())),
            preferred_element_type=jnp.float32,
        ).astype(jnp.bfloat16)


def outer(sinks, query, kvc, low, high, post, taps, inner_attended, out_mine, out_other):
    return pl.pallas_call(
        outer_kernel,
        out_shape=(
            *([jax.ShapeDtypeStruct((128, 2048), jnp.bfloat16)] * 4),
            jax.ShapeDtypeStruct((256, 4), jnp.float32),
        ),
        in_specs=[SMEM] + [VMEM] * 9,
        out_specs=(VMEM,) * 5,
        scratch_shapes=[pltpu.VMEM((512, 512), jnp.bfloat16), pltpu.VMEM((2048, 512), jnp.bfloat16)],
        compiler_params=PARAMS,
        cost_estimate=pl.CostEstimate(
            flops=2 * 512 * 512 * 2048, bytes_accessed=8_000_000, transcendentals=400_000
        ),
    )(sinks, query, kvc, low, high, post, taps, inner_attended, out_mine, out_other)


def halo(block, width):
    count = lax.axis_size(SP)
    forward = [(i, i + 1) for i in range(count - 1)]
    backward = [(i + 1, i) for i in range(count - 1)]
    low = lax.ppermute(block[-width:], SP, forward)
    high = lax.ppermute(block[:width], SP, backward)
    return low, high


def rotation_tables(rows):
    positions = lax.axis_index(SP) * rows + jnp.arange(rows, dtype=jnp.int32)
    half_dim = HEAD_DIM // 2
    inv_freq = rope_base ** (-jnp.arange(0, half_dim, 2).astype(jnp.float32) / half_dim)
    row_angle = (positions // GRID_W).astype(jnp.float32)[:, None] * inv_freq
    col_angle = (positions % GRID_W).astype(jnp.float32)[:, None] * inv_freq
    angle = jnp.concatenate([row_angle, row_angle, col_angle, col_angle] * 2, axis=1)
    lane = lax.broadcasted_iota(jnp.int32, angle.shape, 1)
    sine = jnp.sin(angle)
    return jnp.cos(angle), jnp.where(lane % 32 < 16, -sine, sine)


def on_device(
    tokens,
    norm_gain,
    w_query,
    w_key,
    w_value,
    w_post_gate,
    w_pre_gate,
    w_conv_in,
    conv_taps,
    sink_logit,
    w_out_attn,
    w_out_conv,
):
    rows = tokens.shape[0]
    piece = jnp.concatenate(
        [
            w_key,
            w_value,
            w_pre_gate,
            w_conv_in,
            w_query,
            w_post_gate,
            w_out_attn.T,
            w_out_conv.T,
        ],
        axis=1,
    )
    far_tokens = from_offset(tokens, "tp", 2)
    own = sent_to_all(sent_to_all(piece, "z_high"), "z_low")
    late_tokens = after(tokens, own)
    up_tokens = from_offset(late_tokens, "tp", 1)
    down_tokens = from_offset(late_tokens, "tp", 3)
    normed = normalized(norm_gain[None], [tokens, up_tokens, far_tokens, down_tokens])
    in_parts = with_other_core(across(own[..., :1152]))
    out_own = after(own[..., 1152:], in_parts[4])
    out_across = across(out_own)
    cosine, sine = rotation_tables(rows)
    kvc, query, post = project(normed, cosine, sine, in_parts)
    low, high = halo(kvc, WINDOW)
    out_mine = jnp.stack([after(part, kvc) for part in out_across])
    out_other = from_offset(out_mine, CORE, 1)
    inner_attended, inner_log = inner(sink_logit, query, kvc)
    *outs, outer_log = outer(
        sink_logit, query, kvc, low, high, post, conv_taps, inner_attended, out_mine, out_other
    )
    arrived = [from_offset(outs[step], "tp", -step) for step in (2, 1, 3)]
    total = outs[0].astype(jnp.float32)
    for block in arrived:
        total = total + block.astype(jnp.float32)
    log_sum = jnp.concatenate([outer_log[:WINDOW], inner_log, outer_log[WINDOW:]])
    return (total.astype(jnp.bfloat16), log_sum.T)


def solution(mesh):
    torus = Mesh(mesh.devices.reshape(4, 4, 4, 2, mesh.shape["tp"]), SP_TP)
    return jax.shard_map(
        on_device,
        mesh=torus,
        in_specs=(
            P(SP, "tp"),
            P(),
            P(SP, "tp"),
            P(SP, "tp"),
            P(SP, "tp"),
            P(SP, "tp"),
            P(SP, "tp"),
            P(SP, "tp"),
            P(None, "tp"),
            P("tp"),
            P("tp", SP),
            P("tp", SP),
        ),
        out_specs=(P(SP_TP, None), P("tp", SP)),
        check_vma=False,
    )
```

```python
import jax
import jax.numpy as jnp
from jax import lax
from jax.experimental import pallas as pl
from jax.experimental.pallas import tpu as pltpu
from jax.sharding import Mesh
from jax.sharding import PartitionSpec as P

HEAD_DIM = 64
WINDOW = 128
GRID_W = 64
TOKENS = 65536
SP = ("sp_0", "sp_1", "sp_2")
SP_TP = (*SP, "tp")


rope_base = 10000.0
norm_eps = 1e-06


Z, X, CORE = "sp_0", "sp_1", "sp_2"
VMEM = pl.BlockSpec(memory_space=pltpu.VMEM)
SMEM = pl.BlockSpec(memory_space=pltpu.SMEM)
PARAMS = pltpu.CompilerParams(vmem_limit_bytes=24 * 1024 * 1024)


def from_offset(x, axis, offset):
    count = lax.axis_size(axis)
    return lax.ppermute(x, axis, [((i + offset) % count, i) for i in range(count)])


def after(x, other):
    return lax.optimization_barrier((x, other))[0]


def gathered_parts(own, tables):
    up, far, down = (from_offset(own, X, step) for step in (1, 2, 3))
    near = [from_offset(part, CORE, 1) for part in (after(own, tables), up, down)]
    last = from_offset(after(far, (up, down)), CORE, 1)
    return (own, up, far, down, near[0], near[1], last, near[2])


def norm_kernel(gain_ref, *refs):
    tokens, normed_ref = refs[:4], refs[4]
    tp = lax.axis_index("tp")
    rows, width = tokens[0].shape
    step_rows = 64

    def norm_step(step, carry):
        at = pl.ds(pl.multiple_of(step * step_rows, step_rows), step_rows)
        blocks = [ref[at, :].astype(jnp.float32) for ref in tokens]
        square = sum(jnp.sum(b * b, axis=1, keepdims=True) for b in blocks)
        scale = lax.rsqrt(square / (4 * width) + norm_eps)
        for k, b in enumerate(blocks):
            cols = pl.ds(pl.multiple_of(lax.rem(tp + k, 4) * width, width), width)
            normed_ref[at, cols] = (b * scale * gain_ref[:, cols]).astype(jnp.bfloat16)
        return carry

    lax.fori_loop(0, rows // step_rows, norm_step, 0)


def normalized(gain, tokens):
    rows, width = tokens[0].shape
    return pl.pallas_call(
        norm_kernel,
        out_shape=jax.ShapeDtypeStruct((rows, 4 * width), jnp.bfloat16),
        in_specs=[VMEM] * 5,
        out_specs=VMEM,
        compiler_params=PARAMS,
        cost_estimate=pl.CostEstimate(
            flops=500_000_000, bytes_accessed=4_000_000, transcendentals=512
        ),
    )(gain, *tokens)


def place_rows(parts, out_ref, columns):
    x, core = lax.axis_index(X), lax.axis_index(CORE)
    for side in range(2):
        for x_rel in range(4):
            ref = parts[4 * side + x_rel]
            place = lax.rem(x + x_rel, 4) * 2 + lax.rem(core + side, 2)
            for z in range(16):
                at = pl.ds(pl.multiple_of(z * 128 + place * 16, 16), 16)
                out_ref[at, :] = ref[z, :, columns]


def rotated(x, cosine, sine):
    width = x.shape[-1]
    lane = lax.broadcasted_iota(jnp.int32, x.shape, 1)
    ahead = pltpu.roll(x, width - 16, 1)
    behind = pltpu.roll(x, 16, 1)
    return x * cosine + jnp.where(lane % 32 < 16, ahead, behind) * sine


def project_kernel(*refs):
    normed_ref, cos_ref, sin_ref = refs[:3]
    kvc_ref, query_ref, post_ref, rows_ref = refs[11:]
    place_rows(refs[3:11], rows_ref, slice(0, 1152))

    def projected(first, last):
        return jnp.dot(
            normed_ref[...], rows_ref[:, first:last], preferred_element_type=jnp.float32
        )

    key_value = projected(0, 128)
    lane = lax.broadcasted_iota(jnp.int32, key_value.shape, 1)
    cosine = cos_ref[...]
    sine = sin_ref[...]
    kvc_ref[:, :128] = jnp.where(
        lane < 64, rotated(key_value, cosine, sine), key_value
    ).astype(jnp.bfloat16)
    kvc_ref[:, 128:] = (projected(128, 384) * projected(384, 640)).astype(jnp.bfloat16)
    for half in range(2):
        part = projected(640 + 128 * half, 768 + 128 * half)
        query_ref[:, 128 * half : 128 * (half + 1)] = rotated(part, cosine, sine).astype(
            jnp.bfloat16
        )
    post_ref[...] = projected(896, 1152)


def project(normed, cosine, sine, parts):
    rows = normed.shape[0]
    return pl.pallas_call(
        project_kernel,
        out_shape=(
            jax.ShapeDtypeStruct((rows, 384), jnp.bfloat16),
            jax.ShapeDtypeStruct((rows, 256), jnp.bfloat16),
            jax.ShapeDtypeStruct((rows, 256), jnp.float32),
        ),
        in_specs=[VMEM] * 11,
        out_specs=(VMEM,) * 3,
        scratch_shapes=[pltpu.VMEM((2048, 1152), jnp.bfloat16)],
        compiler_params=PARAMS,
        cost_estimate=pl.CostEstimate(
            flops=2 * rows * 2048 * 1152, bytes_accessed=8_000_000, transcendentals=0
        ),
    )(normed, cosine, sine, *parts)


def attended_block(query, keys, values, sinks, first_key, total):
    heads = query.shape[1] // HEAD_DIM
    stacked = jnp.concatenate(
        [query[:, HEAD_DIM * h : HEAD_DIM * (h + 1)] for h in range(heads)], axis=0
    )
    scores = lax.dot_general(
        stacked, keys, (((1,), (1,)), ((), ())), preferred_element_type=jnp.float32
    ) * HEAD_DIM ** (-0.5)
    row = lax.broadcasted_iota(jnp.int32, scores.shape, 0) % WINDOW
    col = lax.broadcasted_iota(jnp.int32, scores.shape, 1)
    key_pos = first_key + col
    allowed = (col >= row) & (col <= row + 2 * WINDOW) & (key_pos >= 0) & (key_pos < total)
    scores = jnp.where(allowed, scores, -jnp.inf)
    sink = jnp.concatenate([jnp.full((WINDOW, 1), s, jnp.float32) for s in sinks], axis=0)
    row_max = jnp.maximum(jnp.max(scores, axis=1, keepdims=True), sink)
    exp_scores = jnp.exp(scores - row_max)
    denominator = jnp.sum(exp_scores, axis=1, keepdims=True) + jnp.exp(sink - row_max)
    weights = (exp_scores / denominator).astype(jnp.bfloat16)
    result = jnp.dot(weights, values, preferred_element_type=jnp.float32).astype(jnp.bfloat16)
    log_sum = row_max + jnp.log(denominator)
    by_head = [slice(WINDOW * h, WINDOW * (h + 1)) for h in range(heads)]
    return (
        jnp.concatenate([result[s] for s in by_head], axis=1),
        jnp.concatenate([log_sum[s] for s in by_head], axis=1),
    )


def first_position():
    return lax.axis_index(SP) * 512


def inner_kernel(sink_ref, query_ref, kvc_ref, *refs):
    attended_ref, log_ref, out_rows_ref = refs[8:]
    place_rows(refs[:8], out_rows_ref, slice(1152, 1664))
    sinks = [sink_ref[h] for h in range(4)]
    offset = first_position()
    for n in (1, 2):
        window = slice((n - 1) * WINDOW, (n + 2) * WINDOW)
        result, log_sum = attended_block(
            query_ref[n * WINDOW : (n + 1) * WINDOW, :],
            kvc_ref[window, :HEAD_DIM],
            kvc_ref[window, HEAD_DIM : 2 * HEAD_DIM],
            sinks,
            offset + (n - 1) * WINDOW,
            TOKENS,
        )
        attended_ref[(n - 1) * WINDOW : n * WINDOW, :] = result
        log_ref[(n - 1) * WINDOW : n * WINDOW, :] = log_sum


def inner(sinks, query, kvc, parts):
    return pl.pallas_call(
        inner_kernel,
        out_shape=(
            jax.ShapeDtypeStruct((256, 256), jnp.bfloat16),
            jax.ShapeDtypeStruct((256, 4), jnp.float32),
            jax.ShapeDtypeStruct((2048, 512), jnp.bfloat16),
        ),
        in_specs=[SMEM] + [VMEM] * 10,
        out_specs=(VMEM,) * 3,
        compiler_params=PARAMS,
        cost_estimate=pl.CostEstimate(
            flops=2 * 2 * 1024 * 384 * 64 * 20, bytes_accessed=2_000_000, transcendentals=400_000
        ),
    )(sinks, query, kvc, *parts)


def outer_kernel(
    sink_ref, query_ref, kvc_ref, low_ref, high_ref, post_ref, taps_ref, inner_ref, out_rows_ref,
    *refs,
):
    outs, log_ref, both_ref = refs[:4], refs[4], refs[5]
    sinks = [sink_ref[h] for h in range(4)]
    offset = first_position()
    rows = query_ref.shape[0]
    edges = (
        (0, jnp.concatenate([low_ref[:, :128], kvc_ref[: 2 * WINDOW, :128]], axis=0)),
        (3, jnp.concatenate([kvc_ref[rows - 2 * WINDOW :, :128], high_ref[:, :128]], axis=0)),
    )
    for k, (n, window) in enumerate(edges):
        result, log_sum = attended_block(
            query_ref[n * WINDOW : (n + 1) * WINDOW, :],
            window[:, :HEAD_DIM],
            window[:, HEAD_DIM:],
            sinks,
            offset + (n - 1) * WINDOW,
            TOKENS,
        )
        both_ref[n * WINDOW : (n + 1) * WINDOW, :256] = result
        log_ref[k * WINDOW : (k + 1) * WINDOW, :] = log_sum
    both_ref[WINDOW : 3 * WINDOW, :256] = inner_ref[...]
    conv = kvc_ref[:, 128:].astype(jnp.float32)
    row = lax.broadcasted_iota(jnp.int32, conv.shape, 0)
    before = low_ref[WINDOW - 16 :, 128:].astype(jnp.float32)[15:16]
    after = high_ref[:16, 128:].astype(jnp.float32)[0:1]
    previous = jnp.where(row == 0, before, pltpu.roll(conv, 1, 0))
    following = jnp.where(row == rows - 1, after, pltpu.roll(conv, rows - 1, 0))
    convolved = taps_ref[0:1] * previous + taps_ref[1:2] * conv + taps_ref[2:3] * following
    both_ref[:, 256:] = (post_ref[...] * convolved).astype(jnp.bfloat16)
    tp = lax.axis_index("tp")
    for step in (2, 1, 3, 0):
        at = pl.ds(pl.multiple_of(lax.rem(tp + step, 4) * WINDOW, WINDOW), WINDOW)
        outs[step][...] = lax.dot_general(
            both_ref[at, :],
            out_rows_ref[...],
            (((1,), (1,)), ((), ())),
            preferred_element_type=jnp.float32,
        ).astype(jnp.bfloat16)


def outer(sinks, query, kvc, low, high, post, taps, inner_attended, out_rows):
    return pl.pallas_call(
        outer_kernel,
        out_shape=(
            *([jax.ShapeDtypeStruct((128, 2048), jnp.bfloat16)] * 4),
            jax.ShapeDtypeStruct((256, 4), jnp.float32),
        ),
        in_specs=[SMEM] + [VMEM] * 8,
        out_specs=(VMEM,) * 5,
        scratch_shapes=[pltpu.VMEM((512, 512), jnp.bfloat16)],
        compiler_params=PARAMS,
        cost_estimate=pl.CostEstimate(
            flops=2 * 512 * 512 * 2048, bytes_accessed=8_000_000, transcendentals=400_000
        ),
    )(sinks, query, kvc, low, high, post, taps, inner_attended, out_rows)


def halo(block, width):
    count = lax.axis_size(SP)
    forward = [(i, i + 1) for i in range(count - 1)]
    backward = [(i + 1, i) for i in range(count - 1)]
    low = lax.ppermute(block[-width:], SP, forward)
    high = lax.ppermute(block[:width], SP, backward)
    return low, high


def rotation_tables(rows):
    shape = (rows, 2 * HEAD_DIM)
    lane = lax.broadcasted_iota(jnp.int32, shape, 1)
    position = lax.axis_index(SP) * rows + lax.broadcasted_iota(jnp.int32, shape, 0)
    half_dim = HEAD_DIM // 2
    inv_freq = rope_base ** (-(2 * (lane % 16)).astype(jnp.float32) / half_dim)
    index = jnp.where(lane % HEAD_DIM < half_dim, position // GRID_W, position % GRID_W)
    angle = index.astype(jnp.float32) * inv_freq
    sine = jnp.sin(angle)
    return jnp.cos(angle), jnp.where(lane % half_dim < 16, -sine, sine)


def on_device(
    tokens,
    norm_gain,
    w_query,
    w_key,
    w_value,
    w_post_gate,
    w_pre_gate,
    w_conv_in,
    conv_taps,
    sink_logit,
    w_out_attn,
    w_out_conv,
):
    rows = tokens.shape[0]
    piece = jnp.concatenate(
        [
            w_key,
            w_value,
            w_pre_gate,
            w_conv_in,
            w_query,
            w_post_gate,
            w_out_attn.T,
            w_out_conv.T,
        ],
        axis=1,
    )
    own = lax.all_gather(piece, Z, axis=0)
    cosine, sine = rotation_tables(rows)
    parts = gathered_parts(own, (cosine, sine))
    late_tokens = after(tokens, own)
    normed = normalized(
        norm_gain[None], [tokens, *(from_offset(late_tokens, "tp", step) for step in (1, 2, 3))]
    )
    kvc, query, post = project(normed, cosine, sine, parts)
    low, high = halo(kvc, WINDOW)
    inner_attended, inner_log, out_rows = inner(sink_logit, query, kvc, parts)
    *outs, outer_log = outer(
        sink_logit, query, kvc, low, high, post, conv_taps, inner_attended, out_rows
    )
    arrived = [from_offset(outs[step], "tp", -step) for step in (2, 1, 3)]
    total = outs[0].astype(jnp.float32)
    for block in arrived:
        total = total + block.astype(jnp.float32)
    log_sum = jnp.concatenate([outer_log[:WINDOW], inner_log, outer_log[WINDOW:]])
    return (total.astype(jnp.bfloat16), log_sum.T)


def solution(mesh):
    torus = Mesh(mesh.devices.reshape(16, 4, 2, mesh.shape["tp"]), SP_TP)
    return jax.shard_map(
        on_device,
        mesh=torus,
        in_specs=(
            P(SP, "tp"),
            P(),
            P(SP, "tp"),
            P(SP, "tp"),
            P(SP, "tp"),
            P(SP, "tp"),
            P(SP, "tp"),
            P(SP, "tp"),
            P(None, "tp"),
            P("tp"),
            P("tp", SP),
            P("tp", SP),
        ),
        out_specs=(P(SP_TP, None), P("tp", SP)),
        check_vma=False,
    )
```

```python
import jax
import jax.numpy as jnp
from jax import lax
from jax.experimental import pallas as pl
from jax.experimental.pallas import tpu as pltpu
from jax.sharding import Mesh
from jax.sharding import PartitionSpec as P


HEAD_DIM = 64
WINDOW = 128
GRID_W = 64
TOKENS = 65536
SP = ("sp_0", "sp_1", "sp_2")
SP_TP = (*SP, "tp")


rope_base = 10000.0
norm_eps = 1e-06


Z, X, CORE = "sp_0", "sp_1", "sp_2"
VMEM = pl.BlockSpec(memory_space=pltpu.VMEM)
SMEM = pl.BlockSpec(memory_space=pltpu.SMEM)
PARAMS = pltpu.CompilerParams(vmem_limit_bytes=24 * 1024 * 1024)


def from_offset(x, axis, offset):
    count = lax.axis_size(axis)
    return lax.ppermute(x, axis, [((i + offset) % count, i) for i in range(count)])


def after(x, other):
    return lax.optimization_barrier((x, other))[0]


def gathered_parts(own):
    far, up, down = (from_offset(own, X, step) for step in (2, 1, 3))
    mine = (own, up, far, down)
    swapped = []
    for part in mine:
        swapped.append(from_offset(part, CORE, 1))
    return (*mine, *swapped)


def norm_kernel(gain_ref, *refs):
    tokens, normed_ref = refs[:4], refs[4]
    tp = lax.axis_index("tp")
    rows, width = tokens[0].shape
    step_rows = 64

    def norm_step(step, carry):
        at = pl.ds(pl.multiple_of(step * step_rows, step_rows), step_rows)
        blocks = [ref[at, :].astype(jnp.float32) for ref in tokens]
        square = sum(jnp.sum(b * b, axis=1, keepdims=True) for b in blocks)
        scale = lax.rsqrt(square / (4 * width) + norm_eps)
        for k, b in enumerate(blocks):
            cols = pl.ds(pl.multiple_of(lax.rem(tp + k, 4) * width, width), width)
            normed_ref[at, cols] = (b * scale * gain_ref[:, cols]).astype(jnp.bfloat16)
        return carry

    lax.fori_loop(0, rows // step_rows, norm_step, 0)


def normalized(gain, tokens):
    rows, width = tokens[0].shape
    return pl.pallas_call(
        norm_kernel,
        out_shape=jax.ShapeDtypeStruct((rows, 4 * width), jnp.bfloat16),
        in_specs=[VMEM] * 5,
        out_specs=VMEM,
        compiler_params=PARAMS,
        cost_estimate=pl.CostEstimate(
            flops=500_000_000, bytes_accessed=4_000_000, transcendentals=512
        ),
    )(gain, *tokens)


def place_rows(parts, out_ref, columns):
    x, core = lax.axis_index(X), lax.axis_index(CORE)
    for side in range(2):
        for x_rel in range(4):
            ref = parts[4 * side + x_rel]
            place = lax.rem(x + x_rel, 4) * 2 + lax.rem(core + side, 2)
            for z in range(16):
                at = pl.ds(pl.multiple_of(z * 128 + place * 16, 16), 16)
                out_ref[at, :] = ref[z, :, columns]


def rotated(x, cosine, sine):
    width = x.shape[-1]
    lane = lax.broadcasted_iota(jnp.int32, x.shape, 1)
    ahead = pltpu.roll(x, width - 16, 1)
    behind = pltpu.roll(x, 16, 1)
    return x * cosine + jnp.where(lane % 32 < 16, ahead, behind) * sine


def project_kernel(*refs):
    normed_ref, cos_ref, sin_ref = refs[:3]
    kvc_ref, query_ref, post_ref, rows_ref = refs[11:]
    place_rows(refs[3:11], rows_ref, slice(0, 1152))

    def projected(first, last):
        return jnp.dot(
            normed_ref[...], rows_ref[:, first:last], preferred_element_type=jnp.float32
        )

    key_value = projected(0, 128)
    lane = lax.broadcasted_iota(jnp.int32, key_value.shape, 1)
    cosine = cos_ref[...]
    sine = sin_ref[...]
    kvc_ref[:, :128] = jnp.where(
        lane < 64, rotated(key_value, cosine, sine), key_value
    ).astype(jnp.bfloat16)
    kvc_ref[:, 128:] = (projected(128, 384) * projected(384, 640)).astype(jnp.bfloat16)
    for half in range(2):
        part = projected(640 + 128 * half, 768 + 128 * half)
        query_ref[:, 128 * half : 128 * (half + 1)] = rotated(part, cosine, sine).astype(
            jnp.bfloat16
        )
    post_ref[...] = projected(896, 1152)


def project(normed, cosine, sine, parts):
    rows = normed.shape[0]
    return pl.pallas_call(
        project_kernel,
        out_shape=(
            jax.ShapeDtypeStruct((rows, 384), jnp.bfloat16),
            jax.ShapeDtypeStruct((rows, 256), jnp.bfloat16),
            jax.ShapeDtypeStruct((rows, 256), jnp.float32),
        ),
        in_specs=[VMEM] * 11,
        out_specs=(VMEM,) * 3,
        scratch_shapes=[pltpu.VMEM((2048, 1152), jnp.bfloat16)],
        compiler_params=PARAMS,
        cost_estimate=pl.CostEstimate(
            flops=2 * rows * 2048 * 1152, bytes_accessed=8_000_000, transcendentals=0
        ),
    )(normed, cosine, sine, *parts)


def attended_block(query, keys, values, sinks, first_key, total):
    heads = query.shape[1] // HEAD_DIM
    stacked = jnp.concatenate(
        [query[:, HEAD_DIM * h : HEAD_DIM * (h + 1)] for h in range(heads)], axis=0
    )
    scores = lax.dot_general(
        stacked, keys, (((1,), (1,)), ((), ())), preferred_element_type=jnp.float32
    ) * HEAD_DIM ** (-0.5)
    row = lax.broadcasted_iota(jnp.int32, scores.shape, 0) % WINDOW
    col = lax.broadcasted_iota(jnp.int32, scores.shape, 1)
    key_pos = first_key + col
    allowed = (col >= row) & (col <= row + 2 * WINDOW) & (key_pos >= 0) & (key_pos < total)
    scores = jnp.where(allowed, scores, -jnp.inf)
    sink = jnp.concatenate([jnp.full((WINDOW, 1), s, jnp.float32) for s in sinks], axis=0)
    row_max = jnp.maximum(jnp.max(scores, axis=1, keepdims=True), sink)
    exp_scores = jnp.exp(scores - row_max)
    denominator = jnp.sum(exp_scores, axis=1, keepdims=True) + jnp.exp(sink - row_max)
    weights = (exp_scores / denominator).astype(jnp.bfloat16)
    result = jnp.dot(weights, values, preferred_element_type=jnp.float32).astype(jnp.bfloat16)
    log_sum = row_max + jnp.log(denominator)
    by_head = [slice(WINDOW * h, WINDOW * (h + 1)) for h in range(heads)]
    return (
        jnp.concatenate([result[s] for s in by_head], axis=1),
        jnp.concatenate([log_sum[s] for s in by_head], axis=1),
    )


def first_position():
    return lax.axis_index(SP) * 512


def inner_kernel(sink_ref, query_ref, kvc_ref, *refs):
    attended_ref, log_ref, out_rows_ref = refs[8:]
    place_rows(refs[:8], out_rows_ref, slice(1152, 1664))
    sinks = [sink_ref[h] for h in range(4)]
    offset = first_position()
    for n in (1, 2):
        window = slice((n - 1) * WINDOW, (n + 2) * WINDOW)
        result, log_sum = attended_block(
            query_ref[n * WINDOW : (n + 1) * WINDOW, :],
            kvc_ref[window, :HEAD_DIM],
            kvc_ref[window, HEAD_DIM : 2 * HEAD_DIM],
            sinks,
            offset + (n - 1) * WINDOW,
            TOKENS,
        )
        attended_ref[(n - 1) * WINDOW : n * WINDOW, :] = result
        log_ref[(n - 1) * WINDOW : n * WINDOW, :] = log_sum


def inner(sinks, query, kvc, parts):
    return pl.pallas_call(
        inner_kernel,
        out_shape=(
            jax.ShapeDtypeStruct((256, 256), jnp.bfloat16),
            jax.ShapeDtypeStruct((256, 4), jnp.float32),
            jax.ShapeDtypeStruct((2048, 512), jnp.bfloat16),
        ),
        in_specs=[SMEM] + [VMEM] * 10,
        out_specs=(VMEM,) * 3,
        compiler_params=PARAMS,
        cost_estimate=pl.CostEstimate(
            flops=2 * 2 * 1024 * 384 * 64 * 20, bytes_accessed=2_000_000, transcendentals=400_000
        ),
    )(sinks, query, kvc, *parts)


def outer_kernel(
    sink_ref, query_ref, kvc_ref, low_ref, high_ref, post_ref, taps_ref, inner_ref, out_rows_ref,
    *refs,
):
    outs, log_ref, both_ref = refs[:4], refs[4], refs[5]
    sinks = [sink_ref[h] for h in range(4)]
    offset = first_position()
    rows = query_ref.shape[0]
    edges = (
        (0, jnp.concatenate([low_ref[:, :128], kvc_ref[: 2 * WINDOW, :128]], axis=0)),
        (3, jnp.concatenate([kvc_ref[rows - 2 * WINDOW :, :128], high_ref[:, :128]], axis=0)),
    )
    for k, (n, window) in enumerate(edges):
        result, log_sum = attended_block(
            query_ref[n * WINDOW : (n + 1) * WINDOW, :],
            window[:, :HEAD_DIM],
            window[:, HEAD_DIM:],
            sinks,
            offset + (n - 1) * WINDOW,
            TOKENS,
        )
        both_ref[n * WINDOW : (n + 1) * WINDOW, :256] = result
        log_ref[k * WINDOW : (k + 1) * WINDOW, :] = log_sum
    both_ref[WINDOW : 3 * WINDOW, :256] = inner_ref[...]
    conv = kvc_ref[:, 128:].astype(jnp.float32)
    row = lax.broadcasted_iota(jnp.int32, conv.shape, 0)
    before = low_ref[WINDOW - 16 :, 128:].astype(jnp.float32)[15:16]
    after = high_ref[:16, 128:].astype(jnp.float32)[0:1]
    previous = jnp.where(row == 0, before, pltpu.roll(conv, 1, 0))
    following = jnp.where(row == rows - 1, after, pltpu.roll(conv, rows - 1, 0))
    convolved = taps_ref[0:1] * previous + taps_ref[1:2] * conv + taps_ref[2:3] * following
    both_ref[:, 256:] = (post_ref[...] * convolved).astype(jnp.bfloat16)
    tp = lax.axis_index("tp")
    for step in (2, 1, 3, 0):
        at = pl.ds(pl.multiple_of(lax.rem(tp + step, 4) * WINDOW, WINDOW), WINDOW)
        outs[step][...] = lax.dot_general(
            both_ref[at, :],
            out_rows_ref[...],
            (((1,), (1,)), ((), ())),
            preferred_element_type=jnp.float32,
        ).astype(jnp.bfloat16)


def outer(sinks, query, kvc, low, high, post, taps, inner_attended, out_rows):
    return pl.pallas_call(
        outer_kernel,
        out_shape=(
            *([jax.ShapeDtypeStruct((128, 2048), jnp.bfloat16)] * 4),
            jax.ShapeDtypeStruct((256, 4), jnp.float32),
        ),
        in_specs=[SMEM] + [VMEM] * 8,
        out_specs=(VMEM,) * 5,
        scratch_shapes=[pltpu.VMEM((512, 512), jnp.bfloat16)],
        compiler_params=PARAMS,
        cost_estimate=pl.CostEstimate(
            flops=2 * 512 * 512 * 2048, bytes_accessed=8_000_000, transcendentals=400_000
        ),
    )(sinks, query, kvc, low, high, post, taps, inner_attended, out_rows)


def halo(block, width):
    count = lax.axis_size(SP)
    forward = [(i, i + 1) for i in range(count - 1)]
    backward = [(i + 1, i) for i in range(count - 1)]
    low = lax.ppermute(block[-width:], SP, forward)
    high = lax.ppermute(block[:width], SP, backward)
    return low, high


def rotation_tables(rows):
    shape = (rows, 2 * HEAD_DIM)
    lane = lax.broadcasted_iota(jnp.int32, shape, 1)
    position = lax.axis_index(SP) * rows + lax.broadcasted_iota(jnp.int32, shape, 0)
    half_dim = HEAD_DIM // 2
    inv_freq = rope_base ** (-(2 * (lane % 16)).astype(jnp.float32) / half_dim)
    index = jnp.where(lane % HEAD_DIM < half_dim, position // GRID_W, position % GRID_W)
    angle = index.astype(jnp.float32) * inv_freq
    sine = jnp.sin(angle)
    return jnp.cos(angle), jnp.where(lane % half_dim < 16, -sine, sine)


def layer(
    tokens,
    norm_gain,
    w_query,
    w_key,
    w_value,
    w_post_gate,
    w_pre_gate,
    w_conv_in,
    conv_taps,
    sink_logit,
    w_out_attn,
    w_out_conv,
):
    rows = tokens.shape[0]
    piece = jnp.concatenate(
        [
            w_key,
            w_value,
            w_pre_gate,
            w_conv_in,
            w_query,
            w_post_gate,
            w_out_attn.T,
            w_out_conv.T,
        ],
        axis=1,
    )
    own = lax.all_gather(piece, Z, axis=0)
    cosine, sine = rotation_tables(rows)
    parts = gathered_parts(own)
    late_tokens = after(tokens, own)
    arrived = [from_offset(late_tokens, "tp", step) for step in (1, 2, 3)]
    normed = normalized(norm_gain[None], [tokens, *arrived])
    kvc, query, post = project(normed, cosine, sine, parts)
    low, high = halo(kvc, WINDOW)
    inner_attended, inner_log, out_rows = inner(sink_logit, query, kvc, parts)
    *outs, outer_log = outer(
        sink_logit, query, kvc, low, high, post, conv_taps, inner_attended, out_rows
    )
    arrived = [from_offset(outs[step], "tp", -step) for step in (2, 1, 3)]
    total = outs[0].astype(jnp.float32)
    for block in arrived:
        total = total + block.astype(jnp.float32)
    log_sum = jnp.concatenate([outer_log[:WINDOW], inner_log, outer_log[WINDOW:]])
    return (total.astype(jnp.bfloat16), log_sum.T)


def solution(mesh):
    torus = Mesh(mesh.devices.reshape(16, 4, 2, mesh.shape["tp"]), SP_TP)
    return jax.shard_map(
        layer,
        mesh=torus,
        in_specs=(
            P(SP, "tp"),
            P(),
            P(SP, "tp"),
            P(SP, "tp"),
            P(SP, "tp"),
            P(SP, "tp"),
            P(SP, "tp"),
            P(SP, "tp"),
            P(None, "tp"),
            P("tp"),
            P("tp", SP),
            P("tp", SP),
        ),
        out_specs=(P(SP_TP, None), P("tp", SP)),
        check_vma=False,
    )
```

```python
import jax
import jax.numpy as jnp
from jax import lax
from jax.experimental import pallas as pl
from jax.experimental.pallas import tpu as pltpu
from jax.sharding import Mesh
from jax.sharding import PartitionSpec as P


HEAD_DIM = 64
WINDOW = 128
GRID_W = 64
TOKENS = 65536
SP = ("sp_0", "sp_1", "sp_2")
SP_TP = (*SP, "tp")


rope_base = 10000.0
norm_eps = 1e-06


Z, X, CORE = "sp_0", "sp_1", "sp_2"
VMEM = pl.BlockSpec(memory_space=pltpu.VMEM)
SMEM = pl.BlockSpec(memory_space=pltpu.SMEM)


def params(mib):
    return pltpu.CompilerParams(vmem_limit_bytes=mib * 1024 * 1024)


def from_offset(x, axis, offset):
    count = lax.axis_size(axis)
    return lax.ppermute(x, axis, [((i + offset) % count, i) for i in range(count)])


def after(x, other):
    return lax.optimization_barrier((x, other))[0]


def gathered_parts(own):
    far, up, down = (from_offset(own, X, step) for step in (2, 1, 3))
    mine = (own, up, far, down)
    swapped = []
    for part in mine:
        swapped.append(from_offset(part, CORE, 1))
    return (*mine, *swapped)


def norm_kernel(gain_ref, *refs):
    tokens, normed_ref = refs[:4], refs[4]
    tp = lax.axis_index("tp")
    rows, width = tokens[0].shape
    step_rows = 64

    def norm_step(step, carry):
        at = pl.ds(pl.multiple_of(step * step_rows, step_rows), step_rows)
        blocks = [ref[at, :].astype(jnp.float32) for ref in tokens]
        square = sum(jnp.sum(b * b, axis=1, keepdims=True) for b in blocks)
        scale = lax.rsqrt(square / (4 * width) + norm_eps)
        for k, b in enumerate(blocks):
            cols = pl.ds(pl.multiple_of(lax.rem(tp + k, 4) * width, width), width)
            normed_ref[at, cols] = (b * scale * gain_ref[:, cols]).astype(jnp.bfloat16)
        return carry

    lax.fori_loop(0, rows // step_rows, norm_step, 0)


def normalized(gain, tokens):
    rows, width = tokens[0].shape
    return pl.pallas_call(
        norm_kernel,
        out_shape=jax.ShapeDtypeStruct((rows, 4 * width), jnp.bfloat16),
        in_specs=[VMEM] * 5,
        out_specs=VMEM,
        compiler_params=params(8),
        cost_estimate=pl.CostEstimate(
            flops=500_000_000, bytes_accessed=4_000_000, transcendentals=512
        ),
    )(gain, *tokens)


def place_rows(parts, out_ref, columns):
    x, core = lax.axis_index(X), lax.axis_index(CORE)
    for side in range(2):
        for x_rel in range(4):
            ref = parts[4 * side + x_rel]
            place = lax.rem(x + x_rel, 4) * 2 + lax.rem(core + side, 2)
            for z in range(16):
                at = pl.ds(pl.multiple_of(z * 128 + place * 16, 16), 16)
                out_ref[at, :] = ref[z, :, columns]


def rotated(x, cosine, sine):
    width = x.shape[-1]
    lane = lax.broadcasted_iota(jnp.int32, x.shape, 1)
    ahead = pltpu.roll(x, width - 16, 1)
    behind = pltpu.roll(x, 16, 1)
    return x * cosine + jnp.where(lane % 32 < 16, ahead, behind) * sine


def project_kernel(*refs):
    normed_ref, cos_ref, sin_ref = refs[:3]
    kvc_ref, query_ref, post_ref, rows_ref = refs[11:]
    place_rows(refs[3:11], rows_ref, slice(0, 1152))

    def projected(first, last):
        return jnp.dot(
            normed_ref[...], rows_ref[:, first:last], preferred_element_type=jnp.float32
        )

    key_value = projected(0, 128)
    lane = lax.broadcasted_iota(jnp.int32, key_value.shape, 1)
    cosine = cos_ref[...]
    sine = sin_ref[...]
    kvc_ref[:, :128] = jnp.where(
        lane < 64, rotated(key_value, cosine, sine), key_value
    ).astype(jnp.bfloat16)
    kvc_ref[:, 128:] = (projected(128, 384) * projected(384, 640)).astype(jnp.bfloat16)
    for half in range(2):
        part = projected(640 + 128 * half, 768 + 128 * half)
        query_ref[:, 128 * half : 128 * (half + 1)] = rotated(part, cosine, sine).astype(
            jnp.bfloat16
        )
    post_ref[...] = projected(896, 1152)


def project(normed, cosine, sine, parts):
    rows = normed.shape[0]
    return pl.pallas_call(
        project_kernel,
        out_shape=(
            jax.ShapeDtypeStruct((rows, 384), jnp.bfloat16),
            jax.ShapeDtypeStruct((rows, 256), jnp.bfloat16),
            jax.ShapeDtypeStruct((rows, 256), jnp.float32),
        ),
        in_specs=[VMEM] * 11,
        out_specs=(VMEM,) * 3,
        scratch_shapes=[pltpu.VMEM((2048, 1152), jnp.bfloat16)],
        compiler_params=params(24),
        cost_estimate=pl.CostEstimate(
            flops=2 * rows * 2048 * 1152, bytes_accessed=8_000_000, transcendentals=0
        ),
    )(normed, cosine, sine, *parts)


def window_bias():
    row = lax.broadcasted_iota(jnp.int32, (WINDOW, 3 * WINDOW), 0)
    col = lax.broadcasted_iota(jnp.int32, (WINDOW, 3 * WINDOW), 1)
    return jnp.where((col >= row) & (col <= row + 2 * WINDOW), 0.0, -jnp.inf)


def inside_sequence(bias, first_key):
    key_pos = first_key + lax.broadcasted_iota(jnp.int32, bias.shape, 1)
    return jnp.where((key_pos >= 0) & (key_pos < TOKENS), bias, -jnp.inf)


def attended_block(query, keys, values, sinks, bias):
    heads = query.shape[1] // HEAD_DIM
    query = query * jnp.bfloat16(HEAD_DIM**-0.5)
    stacked = jnp.concatenate(
        [query[:, HEAD_DIM * h : HEAD_DIM * (h + 1)] for h in range(heads)], axis=0
    )
    scores = lax.dot_general(
        stacked, keys, (((1,), (1,)), ((), ())), preferred_element_type=jnp.float32
    )
    results, logs = [], []
    for h in range(heads):
        own = scores[WINDOW * h : WINDOW * (h + 1)] + bias
        row_max = jnp.maximum(jnp.max(own, axis=1, keepdims=True), sinks[h])
        exp_scores = jnp.exp(own - row_max)
        denominator = jnp.sum(exp_scores, axis=1, keepdims=True) + jnp.exp(sinks[h] - row_max)
        results.append((exp_scores * (1.0 / denominator)).astype(jnp.bfloat16))
        logs.append(row_max + jnp.log(denominator))
    weights = jnp.concatenate(results, axis=0)
    result = jnp.dot(weights, values, preferred_element_type=jnp.float32).astype(jnp.bfloat16)
    return (
        jnp.concatenate([result[WINDOW * h : WINDOW * (h + 1)] for h in range(heads)], axis=1),
        jnp.concatenate(logs, axis=1),
    )


def first_position():
    return lax.axis_index(SP) * 512


def inner_kernel(sink_ref, query_ref, kvc_ref, *refs):
    attended_ref, log_ref, out_rows_ref = refs[8:]
    place_rows(refs[:8], out_rows_ref, slice(1152, 1664))
    sinks = [sink_ref[h] for h in range(4)]
    bias = window_bias()
    for n in (1, 2):
        window = slice((n - 1) * WINDOW, (n + 2) * WINDOW)
        result, log_sum = attended_block(
            query_ref[n * WINDOW : (n + 1) * WINDOW, :],
            kvc_ref[window, :HEAD_DIM],
            kvc_ref[window, HEAD_DIM : 2 * HEAD_DIM],
            sinks,
            bias,
        )
        attended_ref[(n - 1) * WINDOW : n * WINDOW, :] = result
        log_ref[(n - 1) * WINDOW : n * WINDOW, :] = log_sum


def inner(sinks, query, kvc, parts):
    return pl.pallas_call(
        inner_kernel,
        out_shape=(
            jax.ShapeDtypeStruct((256, 256), jnp.bfloat16),
            jax.ShapeDtypeStruct((256, 4), jnp.float32),
            jax.ShapeDtypeStruct((2048, 512), jnp.bfloat16),
        ),
        in_specs=[SMEM] + [VMEM] * 10,
        out_specs=(VMEM,) * 3,
        compiler_params=params(12),
        cost_estimate=pl.CostEstimate(
            flops=2 * 2 * 1024 * 384 * 64 * 20, bytes_accessed=2_000_000, transcendentals=400_000
        ),
    )(sinks, query, kvc, *parts)


def outer_kernel(
    sink_ref, query_ref, kvc_ref, low_ref, high_ref, post_ref, taps_ref, inner_ref, out_rows_ref,
    *refs,
):
    far_ref, both_ref, log_ref = refs
    sinks = [sink_ref[h] for h in range(4)]
    offset = first_position()
    bias = window_bias()
    rows = query_ref.shape[0]
    edges = (
        (0, jnp.concatenate([low_ref[:, :128], kvc_ref[: 2 * WINDOW, :128]], axis=0)),
        (3, jnp.concatenate([kvc_ref[rows - 2 * WINDOW :, :128], high_ref[:, :128]], axis=0)),
    )
    for k, (n, window) in enumerate(edges):
        result, log_sum = attended_block(
            query_ref[n * WINDOW : (n + 1) * WINDOW, :],
            window[:, :HEAD_DIM],
            window[:, HEAD_DIM:],
            sinks,
            inside_sequence(bias, offset + (n - 1) * WINDOW),
        )
        both_ref[n * WINDOW : (n + 1) * WINDOW, :256] = result
        log_ref[k * WINDOW : (k + 1) * WINDOW, :] = log_sum
    both_ref[WINDOW : 3 * WINDOW, :256] = inner_ref[...]
    conv = kvc_ref[:, 128:].astype(jnp.float32)
    row = lax.broadcasted_iota(jnp.int32, conv.shape, 0)
    before = low_ref[WINDOW - 16 :, 128:].astype(jnp.float32)[15:16]
    after = high_ref[:16, 128:].astype(jnp.float32)[0:1]
    previous = jnp.where(row == 0, before, pltpu.roll(conv, 1, 0))
    following = jnp.where(row == rows - 1, after, pltpu.roll(conv, rows - 1, 0))
    convolved = taps_ref[0:1] * previous + taps_ref[1:2] * conv + taps_ref[2:3] * following
    both_ref[:, 256:] = (post_ref[...] * convolved).astype(jnp.bfloat16)
    send_chunk(both_ref, out_rows_ref, far_ref, 2)


def send_chunk(both_ref, out_rows_ref, out_ref, step):
    block = lax.rem(lax.axis_index("tp") + step, 4)
    out_ref[...] = lax.dot_general(
        both_ref[pl.ds(pl.multiple_of(block * WINDOW, WINDOW), WINDOW), :],
        out_rows_ref[...],
        (((1,), (1,)), ((), ())),
        preferred_element_type=jnp.float32,
    ).astype(jnp.bfloat16)


def near_kernel(both_ref, out_rows_ref, up_ref, down_ref):
    send_chunk(both_ref, out_rows_ref, up_ref, 1)
    send_chunk(both_ref, out_rows_ref, down_ref, 3)


def own_kernel(both_ref, out_rows_ref, own_ref):
    send_chunk(both_ref, out_rows_ref, own_ref, 0)


def chunks(kernel, count, both, out_rows):
    return pl.pallas_call(
        kernel,
        out_shape=(jax.ShapeDtypeStruct((128, 2048), jnp.bfloat16),) * count,
        in_specs=[VMEM] * 2,
        out_specs=(VMEM,) * count,
        compiler_params=params(12),
        cost_estimate=pl.CostEstimate(
            flops=count * 2 * 128 * 512 * 2048, bytes_accessed=3_000_000, transcendentals=0
        ),
    )(both, out_rows)


def outer(sinks, query, kvc, low, high, post, taps, inner_attended, out_rows):
    return pl.pallas_call(
        outer_kernel,
        out_shape=(
            jax.ShapeDtypeStruct((128, 2048), jnp.bfloat16),
            jax.ShapeDtypeStruct((512, 512), jnp.bfloat16),
            jax.ShapeDtypeStruct((256, 4), jnp.float32),
        ),
        in_specs=[SMEM] + [VMEM] * 8,
        out_specs=(VMEM,) * 3,
        compiler_params=params(8),
        cost_estimate=pl.CostEstimate(
            flops=2 * 512 * 512 * 2048, bytes_accessed=8_000_000, transcendentals=400_000
        ),
    )(sinks, query, kvc, low, high, post, taps, inner_attended, out_rows)


def halo(block, width):
    count = lax.axis_size(SP)
    forward = [(i, i + 1) for i in range(count - 1)]
    backward = [(i + 1, i) for i in range(count - 1)]
    low = lax.ppermute(block[-width:], SP, forward)
    high = lax.ppermute(block[:width], SP, backward)
    return low, high


def rotation_tables(rows):
    shape = (rows, 2 * HEAD_DIM)
    lane = lax.broadcasted_iota(jnp.int32, shape, 1)
    position = lax.axis_index(SP) * rows + lax.broadcasted_iota(jnp.int32, shape, 0)
    half_dim = HEAD_DIM // 2
    inv_freq = rope_base ** (-(2 * (lane % 16)).astype(jnp.float32) / half_dim)
    index = jnp.where(lane % HEAD_DIM < half_dim, position // GRID_W, position % GRID_W)
    angle = index.astype(jnp.float32) * inv_freq
    sine = jnp.sin(angle)
    return jnp.cos(angle), jnp.where(lane % half_dim < 16, -sine, sine)


def layer(
    tokens,
    norm_gain,
    w_query,
    w_key,
    w_value,
    w_post_gate,
    w_pre_gate,
    w_conv_in,
    conv_taps,
    sink_logit,
    w_out_attn,
    w_out_conv,
):
    rows = tokens.shape[0]
    piece = jnp.concatenate(
        [
            w_key,
            w_value,
            w_pre_gate,
            w_conv_in,
            w_query,
            w_post_gate,
            w_out_attn.T,
            w_out_conv.T,
        ],
        axis=1,
    )
    own = lax.all_gather(piece, Z, axis=0)
    cosine, sine = rotation_tables(rows)
    parts = gathered_parts(own)
    late_tokens = after(tokens, own)
    arrived = [from_offset(late_tokens, "tp", step) for step in (1, 2, 3)]
    normed = normalized(after(norm_gain[None], (cosine, sine)), [tokens, *arrived])
    kvc, query, post = project(normed, cosine, sine, parts)
    low, high = halo(kvc, WINDOW)
    inner_attended, inner_log, out_rows = inner(sink_logit, query, kvc, parts)
    far, both, outer_log = outer(
        sink_logit, query, kvc, low, high, post, conv_taps, inner_attended, out_rows
    )
    arrived = [from_offset(far, "tp", -2)]
    up, down = chunks(near_kernel, 2, both, out_rows)
    arrived += [from_offset(up, "tp", -1), from_offset(down, "tp", -3)]
    (mine,) = chunks(own_kernel, 1, both, out_rows)
    total = mine.astype(jnp.float32)
    for block in arrived:
        total = total + block.astype(jnp.float32)
    log_sum = jnp.concatenate([outer_log[:WINDOW], inner_log, outer_log[WINDOW:]])
    return (total.astype(jnp.bfloat16), log_sum.T)


def solution(mesh):
    torus = Mesh(mesh.devices.reshape(16, 4, 2, mesh.shape["tp"]), SP_TP)
    return jax.shard_map(
        layer,
        mesh=torus,
        in_specs=(
            P(SP, "tp"),
            P(),
            P(SP, "tp"),
            P(SP, "tp"),
            P(SP, "tp"),
            P(SP, "tp"),
            P(SP, "tp"),
            P(SP, "tp"),
            P(None, "tp"),
            P("tp"),
            P("tp", SP),
            P("tp", SP),
        ),
        out_specs=(P(SP_TP, None), P("tp", SP)),
        check_vma=False,
    )
```

```python
import jax
import jax.numpy as jnp
from jax import lax
from jax.experimental import pallas as pl
from jax.experimental.pallas import tpu as pltpu
from jax.sharding import Mesh
from jax.sharding import PartitionSpec as P


HEAD_DIM = 64
WINDOW = 128
GRID_W = 64
TOKENS = 65536
SP = ("sp_0", "sp_1", "sp_2")
SP_TP = (*SP, "tp")


rope_base = 10000.0
norm_eps = 1e-06


Z, X, CORE = "sp_0", "sp_1", "sp_2"
VMEM = pl.BlockSpec(memory_space=pltpu.VMEM)
SMEM = pl.BlockSpec(memory_space=pltpu.SMEM)


def params(mib):
    return pltpu.CompilerParams(vmem_limit_bytes=mib * 1024 * 1024)


def from_offset(x, axis, offset):
    count = lax.axis_size(axis)
    return lax.ppermute(x, axis, [((i + offset) % count, i) for i in range(count)])


def after(x, other):
    return lax.optimization_barrier((x, other))[0]


def gathered_parts(own):
    far, up, down = (from_offset(own, X, step) for step in (2, 1, 3))
    mine = (own, up, far, down)
    swapped = []
    for part in (own, up, far, down):
        swapped.append(from_offset(part, CORE, 1))
    return (*mine, *swapped)


def norm_kernel(gain_ref, *refs):
    tokens, normed_ref = refs[:4], refs[4]
    tp = lax.axis_index("tp")
    rows, width = tokens[0].shape
    step_rows = 64

    def norm_step(step, carry):
        at = pl.ds(pl.multiple_of(step * step_rows, step_rows), step_rows)
        blocks = [ref[at, :].astype(jnp.float32) for ref in tokens]
        square = sum(jnp.sum(b * b, axis=1, keepdims=True) for b in blocks)
        scale = lax.rsqrt(square / (4 * width) + norm_eps)
        for k, b in enumerate(blocks):
            cols = pl.ds(pl.multiple_of(lax.rem(tp + k, 4) * width, width), width)
            normed_ref[at, cols] = (b * scale * gain_ref[:, cols]).astype(jnp.bfloat16)
        return carry

    lax.fori_loop(0, rows // step_rows, norm_step, 0)


def normalized(gain, tokens):
    rows, width = tokens[0].shape
    return pl.pallas_call(
        norm_kernel,
        out_shape=jax.ShapeDtypeStruct((rows, 4 * width), jnp.bfloat16),
        in_specs=[VMEM] * 5,
        out_specs=VMEM,
        compiler_params=params(8),
        cost_estimate=pl.CostEstimate(
            flops=500_000_000, bytes_accessed=4_000_000, transcendentals=512
        ),
    )(gain, *tokens)


def place_rows(parts, out_ref, columns):
    x, core = lax.axis_index(X), lax.axis_index(CORE)
    for side in range(2):
        for x_rel in range(4):
            ref = parts[4 * side + x_rel]
            place = lax.rem(x + x_rel, 4) * 2 + lax.rem(core + side, 2)
            for z in range(16):
                at = pl.ds(pl.multiple_of(z * 128 + place * 16, 16), 16)
                out_ref[at, :] = ref[z, :, columns]


def rotated(x, cosine, sine):
    width = x.shape[-1]
    lane = lax.broadcasted_iota(jnp.int32, x.shape, 1)
    ahead = pltpu.roll(x, width - 16, 1)
    behind = pltpu.roll(x, 16, 1)
    return x * cosine + jnp.where(lane % 32 < 16, ahead, behind) * sine


def project_kernel(*refs):
    normed_ref, cos_ref, sin_ref = refs[:3]
    kvc_ref, query_ref, post_ref, out_rows_ref, rows_ref = refs[11:]
    place_rows(refs[3:11], rows_ref, slice(0, 1152))
    place_rows(refs[3:11], out_rows_ref, slice(1152, 1664))

    def projected(first, last):
        return jnp.dot(
            normed_ref[...], rows_ref[:, first:last], preferred_element_type=jnp.float32
        )

    key_value = projected(0, 128)
    lane = lax.broadcasted_iota(jnp.int32, key_value.shape, 1)
    cosine = cos_ref[...]
    sine = sin_ref[...]
    kvc_ref[:, :128] = jnp.where(
        lane < 64, rotated(key_value, cosine, sine), key_value
    ).astype(jnp.bfloat16)
    kvc_ref[:, 128:] = (projected(128, 384) * projected(384, 640)).astype(jnp.bfloat16)
    for half in range(2):
        part = projected(640 + 128 * half, 768 + 128 * half)
        query_ref[:, 128 * half : 128 * (half + 1)] = rotated(part, cosine, sine).astype(
            jnp.bfloat16
        )
    post_ref[...] = projected(896, 1152)


def project(normed, cosine, sine, parts):
    rows = normed.shape[0]
    return pl.pallas_call(
        project_kernel,
        out_shape=(
            jax.ShapeDtypeStruct((rows, 384), jnp.bfloat16),
            jax.ShapeDtypeStruct((rows, 256), jnp.bfloat16),
            jax.ShapeDtypeStruct((rows, 256), jnp.float32),
            jax.ShapeDtypeStruct((2048, 512), jnp.bfloat16),
        ),
        in_specs=[VMEM] * 11,
        out_specs=(VMEM,) * 4,
        scratch_shapes=[pltpu.VMEM((2048, 1152), jnp.bfloat16)],
        compiler_params=params(24),
        cost_estimate=pl.CostEstimate(
            flops=2 * rows * 2048 * 1152, bytes_accessed=8_000_000, transcendentals=0
        ),
    )(normed, cosine, sine, *parts)


def window_bias():
    row = lax.broadcasted_iota(jnp.int32, (WINDOW, 3 * WINDOW), 0)
    col = lax.broadcasted_iota(jnp.int32, (WINDOW, 3 * WINDOW), 1)
    return jnp.where((col >= row) & (col <= row + 2 * WINDOW), 0.0, -jnp.inf)


def inside_sequence(bias, first_key):
    key_pos = first_key + lax.broadcasted_iota(jnp.int32, bias.shape, 1)
    return jnp.where((key_pos >= 0) & (key_pos < TOKENS), bias, -jnp.inf)


def attended_block(query, keys, values, sinks, bias):
    heads = query.shape[1] // HEAD_DIM
    query = query * jnp.bfloat16(HEAD_DIM**-0.5)
    stacked = jnp.concatenate(
        [query[:, HEAD_DIM * h : HEAD_DIM * (h + 1)] for h in range(heads)], axis=0
    )
    scores = lax.dot_general(
        stacked, keys, (((1,), (1,)), ((), ())), preferred_element_type=jnp.float32
    )
    results, logs = [], []
    for h in range(heads):
        own = scores[WINDOW * h : WINDOW * (h + 1)] + bias
        row_max = jnp.maximum(jnp.max(own, axis=1, keepdims=True), sinks[h])
        exp_scores = jnp.exp(own - row_max)
        denominator = jnp.sum(exp_scores, axis=1, keepdims=True) + jnp.exp(sinks[h] - row_max)
        results.append((exp_scores * (1.0 / denominator)).astype(jnp.bfloat16))
        logs.append(row_max + jnp.log(denominator))
    weights = jnp.concatenate(results, axis=0)
    result = jnp.dot(weights, values, preferred_element_type=jnp.float32).astype(jnp.bfloat16)
    return (
        jnp.concatenate([result[WINDOW * h : WINDOW * (h + 1)] for h in range(heads)], axis=1),
        jnp.concatenate(logs, axis=1),
    )


def first_position():
    return lax.axis_index(SP) * 512


def inner_kernel(sink_ref, query_ref, kvc_ref, attended_ref, log_ref):
    sinks = [sink_ref[h] for h in range(4)]
    bias = window_bias()
    for n in (1, 2):
        window = slice((n - 1) * WINDOW, (n + 2) * WINDOW)
        result, log_sum = attended_block(
            query_ref[n * WINDOW : (n + 1) * WINDOW, :],
            kvc_ref[window, :HEAD_DIM],
            kvc_ref[window, HEAD_DIM : 2 * HEAD_DIM],
            sinks,
            bias,
        )
        attended_ref[(n - 1) * WINDOW : n * WINDOW, :] = result
        log_ref[(n - 1) * WINDOW : n * WINDOW, :] = log_sum


def inner(sinks, query, kvc):
    return pl.pallas_call(
        inner_kernel,
        out_shape=(
            jax.ShapeDtypeStruct((256, 256), jnp.bfloat16),
            jax.ShapeDtypeStruct((256, 4), jnp.float32),
        ),
        in_specs=[SMEM, VMEM, VMEM],
        out_specs=(VMEM, VMEM),
        compiler_params=params(12),
        cost_estimate=pl.CostEstimate(
            flops=2 * 2 * 1024 * 384 * 64 * 20, bytes_accessed=2_000_000, transcendentals=400_000
        ),
    )(sinks, query, kvc)


def outer_kernel(
    sink_ref, query_ref, kvc_ref, low_ref, high_ref, post_ref, taps_ref, inner_ref, out_rows_ref,
    *refs,
):
    far_ref, both_ref, log_ref = refs
    sinks = [sink_ref[h] for h in range(4)]
    offset = first_position()
    bias = window_bias()
    rows = query_ref.shape[0]
    edges = (
        (0, jnp.concatenate([low_ref[:, :128], kvc_ref[: 2 * WINDOW, :128]], axis=0)),
        (3, jnp.concatenate([kvc_ref[rows - 2 * WINDOW :, :128], high_ref[:, :128]], axis=0)),
    )
    for k, (n, window) in enumerate(edges):
        result, log_sum = attended_block(
            query_ref[n * WINDOW : (n + 1) * WINDOW, :],
            window[:, :HEAD_DIM],
            window[:, HEAD_DIM:],
            sinks,
            inside_sequence(bias, offset + (n - 1) * WINDOW),
        )
        both_ref[n * WINDOW : (n + 1) * WINDOW, :256] = result
        log_ref[k * WINDOW : (k + 1) * WINDOW, :] = log_sum
    both_ref[WINDOW : 3 * WINDOW, :256] = inner_ref[...]
    conv = kvc_ref[:, 128:].astype(jnp.float32)
    row = lax.broadcasted_iota(jnp.int32, conv.shape, 0)
    before = low_ref[WINDOW - 16 :, 128:].astype(jnp.float32)[15:16]
    after = high_ref[:16, 128:].astype(jnp.float32)[0:1]
    previous = jnp.where(row == 0, before, pltpu.roll(conv, 1, 0))
    following = jnp.where(row == rows - 1, after, pltpu.roll(conv, rows - 1, 0))
    convolved = taps_ref[0:1] * previous + taps_ref[1:2] * conv + taps_ref[2:3] * following
    both_ref[:, 256:] = (post_ref[...] * convolved).astype(jnp.bfloat16)
    far = chunk(both_ref, out_rows_ref, 2).astype(jnp.bfloat16)
    half = far.shape[1] // 2
    far_ref[0] = far[:, :half]
    far_ref[1] = far[:, half:]


def chunk(both_ref, out_rows_ref, step):
    block = lax.rem(lax.axis_index("tp") + step, 4)
    return lax.dot_general(
        both_ref[pl.ds(pl.multiple_of(block * WINDOW, WINDOW), WINDOW), :],
        out_rows_ref[...],
        (((1,), (1,)), ((), ())),
        preferred_element_type=jnp.float32,
    )


def near_kernel(both_ref, out_rows_ref, low_ref, high_ref, up_ref, down_ref):
    half = low_ref.shape[1]
    up = chunk(both_ref, out_rows_ref, 1)
    up_ref[:, :half] = (up[:, :half] + low_ref[...].astype(jnp.float32)).astype(jnp.bfloat16)
    up_ref[:, half:] = up[:, half:].astype(jnp.bfloat16)
    down = chunk(both_ref, out_rows_ref, 3)
    down_ref[:, :half] = down[:, :half].astype(jnp.bfloat16)
    down_ref[:, half:] = (down[:, half:] + high_ref[...].astype(jnp.float32)).astype(jnp.bfloat16)


def own_kernel(both_ref, out_rows_ref, own_ref):
    own_ref[...] = chunk(both_ref, out_rows_ref, 0).astype(jnp.bfloat16)


def chunks(kernel, count, *arrays):
    return pl.pallas_call(
        kernel,
        out_shape=(jax.ShapeDtypeStruct((128, 2048), jnp.bfloat16),) * count,
        in_specs=[VMEM] * len(arrays),
        out_specs=(VMEM,) * count,
        compiler_params=params(12),
        cost_estimate=pl.CostEstimate(
            flops=count * 2 * 128 * 512 * 2048, bytes_accessed=3_000_000, transcendentals=0
        ),
    )(*arrays)


def outer(sinks, query, kvc, low, high, post, taps, inner_attended, out_rows):
    return pl.pallas_call(
        outer_kernel,
        out_shape=(
            jax.ShapeDtypeStruct((2, 128, 1024), jnp.bfloat16),
            jax.ShapeDtypeStruct((512, 512), jnp.bfloat16),
            jax.ShapeDtypeStruct((256, 4), jnp.float32),
        ),
        in_specs=[SMEM] + [VMEM] * 8,
        out_specs=(VMEM,) * 3,
        compiler_params=params(8),
        cost_estimate=pl.CostEstimate(
            flops=2 * 512 * 512 * 2048, bytes_accessed=8_000_000, transcendentals=400_000
        ),
    )(sinks, query, kvc, low, high, post, taps, inner_attended, out_rows)


def halo(block, width):
    count = lax.axis_size(SP)
    forward = [(i, i + 1) for i in range(count - 1)]
    backward = [(i + 1, i) for i in range(count - 1)]
    low = lax.ppermute(block[-width:], SP, forward)
    high = lax.ppermute(block[:width], SP, backward)
    return low, high


def rotation_tables(rows):
    shape = (rows, 2 * HEAD_DIM)
    lane = lax.broadcasted_iota(jnp.int32, shape, 1)
    position = lax.axis_index(SP) * rows + lax.broadcasted_iota(jnp.int32, shape, 0)
    half_dim = HEAD_DIM // 2
    inv_freq = rope_base ** (-(2 * (lane % 16)).astype(jnp.float32) / half_dim)
    index = jnp.where(lane % HEAD_DIM < half_dim, position // GRID_W, position % GRID_W)
    angle = index.astype(jnp.float32) * inv_freq
    sine = jnp.sin(angle)
    return jnp.cos(angle), jnp.where(lane % half_dim < 16, -sine, sine)


def layer(
    tokens,
    norm_gain,
    w_query,
    w_key,
    w_value,
    w_post_gate,
    w_pre_gate,
    w_conv_in,
    conv_taps,
    sink_logit,
    w_out_attn,
    w_out_conv,
):
    rows = tokens.shape[0]
    piece = jnp.concatenate(
        [
            w_key,
            w_value,
            w_pre_gate,
            w_conv_in,
            w_query,
            w_post_gate,
            w_out_attn.T,
            w_out_conv.T,
        ],
        axis=1,
    )
    cosine, sine = rotation_tables(rows)
    own = lax.all_gather(after(piece, (cosine, sine)), Z, axis=0)
    parts = gathered_parts(own)
    late_tokens = after(tokens, own)
    arrived = [from_offset(late_tokens, "tp", step) for step in (1, 2, 3)]
    normed = normalized(norm_gain[None], [tokens, *arrived])
    kvc, query, post, out_rows = project(normed, cosine, sine, parts)
    low, high = halo(kvc, WINDOW)
    inner_attended, inner_log = inner(sink_logit, query, kvc)
    far, both, outer_log = outer(
        sink_logit, query, kvc, low, high, post, conv_taps, inner_attended, out_rows
    )
    low_half = from_offset(far[0], "tp", -1)
    high_half = from_offset(far[1], "tp", 1)
    up, down = chunks(near_kernel, 2, both, out_rows, low_half, high_half)
    arrived = [from_offset(up, "tp", -1), from_offset(down, "tp", 1)]
    (mine,) = chunks(own_kernel, 1, both, out_rows)
    total = mine.astype(jnp.float32)
    for block in arrived:
        total = total + block.astype(jnp.float32)
    log_sum = jnp.concatenate([outer_log[:WINDOW], inner_log, outer_log[WINDOW:]])
    return (total.astype(jnp.bfloat16), log_sum.T)


def solution(mesh):
    torus = Mesh(mesh.devices.reshape(16, 4, 2, mesh.shape["tp"]), SP_TP)
    return jax.shard_map(
        layer,
        mesh=torus,
        in_specs=(
            P(SP, "tp"),
            P(),
            P(SP, "tp"),
            P(SP, "tp"),
            P(SP, "tp"),
            P(SP, "tp"),
            P(SP, "tp"),
            P(SP, "tp"),
            P(None, "tp"),
            P("tp"),
            P("tp", SP),
            P("tp", SP),
        ),
        out_specs=(P(SP_TP, None), P("tp", SP)),
        check_vma=False,
    )
```

```python
import functools

import jax
import jax.numpy as jnp
from jax import lax
from jax.experimental import pallas as pl
from jax.experimental.pallas import tpu as pltpu
from jax.sharding import Mesh
from jax.sharding import PartitionSpec as P


HEAD_DIM = 64
WINDOW = 128
GRID_W = 64
TOKENS = 65536
SP = ("sp_0", "sp_1", "sp_2")
SP_TP = (*SP, "tp")


rope_base = 10000.0
norm_eps = 1e-06


Z, X, CORE = "sp_0", "sp_1", "sp_2"
VMEM = pl.BlockSpec(memory_space=pltpu.VMEM)
SMEM = pl.BlockSpec(memory_space=pltpu.SMEM)


def params(mib):
    return pltpu.CompilerParams(vmem_limit_bytes=mib * 1024 * 1024)


def from_offset(x, axis, offset):
    count = lax.axis_size(axis)
    return lax.ppermute(x, axis, [((i + offset) % count, i) for i in range(count)])


def after(x, other):
    return lax.optimization_barrier((x, other))[0]


def gathered_parts(own):
    far, up, down = (from_offset(own, X, step) for step in (2, 1, 3))
    mine = (own, up, far, down)
    swapped = []
    for part in (own, up, far, down):
        swapped.append(from_offset(part, CORE, 1))
    return (*mine, *swapped)


def stage_kernel(tokens_ref, gain_ref, staged_tokens_ref, staged_gain_ref):
    staged_tokens_ref[...] = tokens_ref[...]
    staged_gain_ref[...] = gain_ref[...]


def staged(tokens, gain):
    return pl.pallas_call(
        stage_kernel,
        out_shape=(
            jax.ShapeDtypeStruct(tokens.shape, tokens.dtype),
            jax.ShapeDtypeStruct(gain.shape, gain.dtype),
        ),
        in_specs=[VMEM] * 2,
        out_specs=(VMEM,) * 2,
        compiler_params=params(4),
        cost_estimate=pl.CostEstimate(flops=500_000, bytes_accessed=1_000_000, transcendentals=0),
    )(tokens, gain)


def norm_kernel(gain_ref, *refs):
    tokens, normed_ref = refs[:4], refs[4]
    tp = lax.axis_index("tp")
    rows, width = tokens[0].shape
    step_rows = 64

    def norm_step(step, carry):
        at = pl.ds(pl.multiple_of(step * step_rows, step_rows), step_rows)
        blocks = [ref[at, :].astype(jnp.float32) for ref in tokens]
        square = sum(jnp.sum(b * b, axis=1, keepdims=True) for b in blocks)
        scale = lax.rsqrt(square / (4 * width) + norm_eps)
        for k, b in enumerate(blocks):
            cols = pl.ds(pl.multiple_of(lax.rem(tp + k, 4) * width, width), width)
            normed_ref[at, cols] = (b * scale * gain_ref[:, cols]).astype(jnp.bfloat16)
        return carry

    lax.fori_loop(0, rows // step_rows, norm_step, 0)


def normalized(gain, tokens):
    rows, width = tokens[0].shape
    return pl.pallas_call(
        norm_kernel,
        out_shape=jax.ShapeDtypeStruct((rows, 4 * width), jnp.bfloat16),
        in_specs=[VMEM] * 5,
        out_specs=VMEM,
        compiler_params=params(8),
        cost_estimate=pl.CostEstimate(
            flops=500_000_000, bytes_accessed=4_000_000, transcendentals=512
        ),
    )(gain, *tokens)


def place_rows(parts, out_ref, columns):
    x, core = lax.axis_index(X), lax.axis_index(CORE)
    for side in range(2):
        for x_rel in range(4):
            ref = parts[4 * side + x_rel]
            place = lax.rem(x + x_rel, 4) * 2 + lax.rem(core + side, 2)
            for z in range(16):
                at = pl.ds(pl.multiple_of(z * 128 + place * 16, 16), 16)
                out_ref[at, :] = ref[z, :, columns]


def rotated(x, cosine, sine):
    width = x.shape[-1]
    lane = lax.broadcasted_iota(jnp.int32, x.shape, 1)
    ahead = pltpu.roll(x, width - 16, 1)
    behind = pltpu.roll(x, 16, 1)
    return x * cosine + jnp.where(lane % 32 < 16, ahead, behind) * sine


def project_kernel(*refs):
    normed_ref, cos_ref, sin_ref = refs[:3]
    kvc_ref, query_ref, post_ref, out_rows_ref, rows_ref = refs[11:]
    place_rows(refs[3:11], rows_ref, slice(0, 1152))
    place_rows(refs[3:11], out_rows_ref, slice(1152, 1664))

    def projected(first, last):
        return jnp.dot(
            normed_ref[...], rows_ref[:, first:last], preferred_element_type=jnp.float32
        )

    key_value = projected(0, 128)
    lane = lax.broadcasted_iota(jnp.int32, key_value.shape, 1)
    cosine = cos_ref[...]
    sine = sin_ref[...]
    kvc_ref[:, :128] = jnp.where(
        lane < 64, rotated(key_value, cosine, sine), key_value
    ).astype(jnp.bfloat16)
    kvc_ref[:, 128:] = (projected(128, 384) * projected(384, 640)).astype(jnp.bfloat16)
    for half in range(2):
        part = projected(640 + 128 * half, 768 + 128 * half)
        query_ref[:, 128 * half : 128 * (half + 1)] = rotated(part, cosine, sine).astype(
            jnp.bfloat16
        )
    post_ref[...] = projected(896, 1152)


def project(normed, cosine, sine, parts):
    rows = normed.shape[0]
    return pl.pallas_call(
        project_kernel,
        out_shape=(
            jax.ShapeDtypeStruct((rows, 384), jnp.bfloat16),
            jax.ShapeDtypeStruct((rows, 256), jnp.bfloat16),
            jax.ShapeDtypeStruct((rows, 256), jnp.float32),
            jax.ShapeDtypeStruct((2048, 512), jnp.bfloat16),
        ),
        in_specs=[VMEM] * 11,
        out_specs=(VMEM,) * 4,
        scratch_shapes=[pltpu.VMEM((2048, 1152), jnp.bfloat16)],
        compiler_params=params(24),
        cost_estimate=pl.CostEstimate(
            flops=2 * rows * 2048 * 1152, bytes_accessed=8_000_000, transcendentals=0
        ),
    )(normed, cosine, sine, *parts)


def window_bias():
    row = lax.broadcasted_iota(jnp.int32, (WINDOW, 3 * WINDOW), 0)
    col = lax.broadcasted_iota(jnp.int32, (WINDOW, 3 * WINDOW), 1)
    return jnp.where((col >= row) & (col <= row + 2 * WINDOW), 0.0, -jnp.inf)


def inside_sequence(bias, first_key):
    key_pos = first_key + lax.broadcasted_iota(jnp.int32, bias.shape, 1)
    return jnp.where((key_pos >= 0) & (key_pos < TOKENS), bias, -jnp.inf)


def attended_block(query, keys, values, sinks, bias):
    heads = query.shape[1] // HEAD_DIM
    query = query * jnp.bfloat16(HEAD_DIM**-0.5)
    stacked = jnp.concatenate(
        [query[:, HEAD_DIM * h : HEAD_DIM * (h + 1)] for h in range(heads)], axis=0
    )
    scores = lax.dot_general(
        stacked, keys, (((1,), (1,)), ((), ())), preferred_element_type=jnp.float32
    )
    results, logs = [], []
    for h in range(heads):
        own = scores[WINDOW * h : WINDOW * (h + 1)] + bias
        row_max = jnp.maximum(jnp.max(own, axis=1, keepdims=True), sinks[h])
        exp_scores = jnp.exp(own - row_max)
        denominator = jnp.sum(exp_scores, axis=1, keepdims=True) + jnp.exp(sinks[h] - row_max)
        results.append((exp_scores * (1.0 / denominator)).astype(jnp.bfloat16))
        logs.append(row_max + jnp.log(denominator))
    weights = jnp.concatenate(results, axis=0)
    result = jnp.dot(weights, values, preferred_element_type=jnp.float32).astype(jnp.bfloat16)
    return (
        jnp.concatenate([result[WINDOW * h : WINDOW * (h + 1)] for h in range(heads)], axis=1),
        jnp.concatenate(logs, axis=1),
    )


def first_position():
    return lax.axis_index(SP) * 512


def inner_kernel(sink_ref, query_ref, kvc_ref, attended_ref, log_ref):
    sinks = [sink_ref[h] for h in range(4)]
    bias = window_bias()
    for n in (1, 2):
        window = slice((n - 1) * WINDOW, (n + 2) * WINDOW)
        result, log_sum = attended_block(
            query_ref[n * WINDOW : (n + 1) * WINDOW, :],
            kvc_ref[window, :HEAD_DIM],
            kvc_ref[window, HEAD_DIM : 2 * HEAD_DIM],
            sinks,
            bias,
        )
        attended_ref[(n - 1) * WINDOW : n * WINDOW, :] = result
        log_ref[(n - 1) * WINDOW : n * WINDOW, :] = log_sum


def inner(sinks, query, kvc):
    return pl.pallas_call(
        inner_kernel,
        out_shape=(
            jax.ShapeDtypeStruct((256, 256), jnp.bfloat16),
            jax.ShapeDtypeStruct((256, 4), jnp.float32),
        ),
        in_specs=[SMEM, VMEM, VMEM],
        out_specs=(VMEM, VMEM),
        compiler_params=params(12),
        cost_estimate=pl.CostEstimate(
            flops=2 * 2 * 1024 * 384 * 64 * 20, bytes_accessed=2_000_000, transcendentals=400_000
        ),
    )(sinks, query, kvc)


def outer_kernel(
    sink_ref, query_ref, kvc_ref, low_ref, high_ref, post_ref, taps_ref, inner_ref, out_rows_ref,
    *refs,
):
    far_ref, both_ref, log_ref = refs
    sinks = [sink_ref[h] for h in range(4)]
    offset = first_position()
    bias = window_bias()
    rows = query_ref.shape[0]
    edges = (
        (0, jnp.concatenate([low_ref[:, :128], kvc_ref[: 2 * WINDOW, :128]], axis=0)),
        (3, jnp.concatenate([kvc_ref[rows - 2 * WINDOW :, :128], high_ref[:, :128]], axis=0)),
    )
    for k, (n, window) in enumerate(edges):
        result, log_sum = attended_block(
            query_ref[n * WINDOW : (n + 1) * WINDOW, :],
            window[:, :HEAD_DIM],
            window[:, HEAD_DIM:],
            sinks,
            inside_sequence(bias, offset + (n - 1) * WINDOW),
        )
        both_ref[n * WINDOW : (n + 1) * WINDOW, :256] = result
        log_ref[k * WINDOW : (k + 1) * WINDOW, :] = log_sum
    both_ref[WINDOW : 3 * WINDOW, :256] = inner_ref[...]
    conv = kvc_ref[:, 128:].astype(jnp.float32)
    row = lax.broadcasted_iota(jnp.int32, conv.shape, 0)
    before = low_ref[WINDOW - 16 :, 128:].astype(jnp.float32)[15:16]
    after = high_ref[:16, 128:].astype(jnp.float32)[0:1]
    previous = jnp.where(row == 0, before, pltpu.roll(conv, 1, 0))
    following = jnp.where(row == rows - 1, after, pltpu.roll(conv, rows - 1, 0))
    convolved = taps_ref[0:1] * previous + taps_ref[1:2] * conv + taps_ref[2:3] * following
    both_ref[:, 256:] = (post_ref[...] * convolved).astype(jnp.bfloat16)
    far_ref[...] = chunk(both_ref, out_rows_ref, 2).astype(jnp.bfloat16)


def chunk(both_ref, out_rows_ref, step):
    block = lax.rem(lax.axis_index("tp") + step, 4)
    return lax.dot_general(
        both_ref[pl.ds(pl.multiple_of(block * WINDOW, WINDOW), WINDOW), :],
        out_rows_ref[...],
        (((1,), (1,)), ((), ())),
        preferred_element_type=jnp.float32,
    )


def chunk_kernel(step, both_ref, out_rows_ref, out_ref):
    out_ref[...] = chunk(both_ref, out_rows_ref, step).astype(jnp.bfloat16)


def total_kernel(*refs):
    total = refs[0][...].astype(jnp.float32)
    for ref in refs[1:-1]:
        total = total + ref[...].astype(jnp.float32)
    refs[-1][...] = total.astype(jnp.bfloat16)


def rows_out(kernel, *arrays):
    return pl.pallas_call(
        kernel,
        out_shape=jax.ShapeDtypeStruct((128, 2048), jnp.bfloat16),
        in_specs=[VMEM] * len(arrays),
        out_specs=VMEM,
        compiler_params=params(12),
        cost_estimate=pl.CostEstimate(
            flops=2 * 128 * 512 * 2048, bytes_accessed=3_000_000, transcendentals=0
        ),
    )(*arrays)


def outer(sinks, query, kvc, low, high, post, taps, inner_attended, out_rows):
    return pl.pallas_call(
        outer_kernel,
        out_shape=(
            jax.ShapeDtypeStruct((128, 2048), jnp.bfloat16),
            jax.ShapeDtypeStruct((512, 512), jnp.bfloat16),
            jax.ShapeDtypeStruct((256, 4), jnp.float32),
        ),
        in_specs=[SMEM] + [VMEM] * 8,
        out_specs=(VMEM,) * 3,
        compiler_params=params(8),
        cost_estimate=pl.CostEstimate(
            flops=2 * 512 * 512 * 2048, bytes_accessed=8_000_000, transcendentals=400_000
        ),
    )(sinks, query, kvc, low, high, post, taps, inner_attended, out_rows)


def halo(block, width):
    count = lax.axis_size(SP)
    forward = [(i, i + 1) for i in range(count - 1)]
    backward = [(i + 1, i) for i in range(count - 1)]
    low = lax.ppermute(block[-width:], SP, forward)
    high = lax.ppermute(block[:width], SP, backward)
    return low, high


def rotation_tables(rows):
    shape = (rows, 2 * HEAD_DIM)
    lane = lax.broadcasted_iota(jnp.int32, shape, 1)
    position = lax.axis_index(SP) * rows + lax.broadcasted_iota(jnp.int32, shape, 0)
    half_dim = HEAD_DIM // 2
    inv_freq = rope_base ** (-(2 * (lane % 16)).astype(jnp.float32) / half_dim)
    index = jnp.where(lane % HEAD_DIM < half_dim, position // GRID_W, position % GRID_W)
    angle = index.astype(jnp.float32) * inv_freq
    sine = jnp.sin(angle)
    return jnp.cos(angle), jnp.where(lane % half_dim < 16, -sine, sine)


def layer(
    tokens,
    norm_gain,
    w_query,
    w_key,
    w_value,
    w_post_gate,
    w_pre_gate,
    w_conv_in,
    conv_taps,
    sink_logit,
    w_out_attn,
    w_out_conv,
):
    rows = tokens.shape[0]
    piece = jnp.concatenate(
        [
            w_key,
            w_value,
            w_pre_gate,
            w_conv_in,
            w_query,
            w_post_gate,
            w_out_attn.T,
            w_out_conv.T,
        ],
        axis=1,
    )
    cosine, sine = rotation_tables(rows)
    own = lax.all_gather(after(piece, (cosine, sine)), Z, axis=0)
    parts = gathered_parts(own)
    late_tokens = after(tokens, own)
    arrived = [from_offset(late_tokens, "tp", step) for step in (1, 2, 3)]
    own_tokens, gain = staged(tokens, norm_gain[None])
    normed = normalized(gain, [own_tokens, *arrived])
    kvc, query, post, out_rows = project(normed, cosine, sine, parts)
    low, high = halo(kvc, WINDOW)
    inner_attended, inner_log = inner(sink_logit, query, kvc)
    far, both, outer_log = outer(
        sink_logit, query, kvc, low, high, post, conv_taps, inner_attended, out_rows
    )
    arrived = [from_offset(far, "tp", -2)]
    up = rows_out(functools.partial(chunk_kernel, 1), both, out_rows)
    arrived.append(from_offset(up, "tp", -1))
    down = rows_out(functools.partial(chunk_kernel, 3), both, out_rows)
    arrived.append(from_offset(down, "tp", 1))
    mine = rows_out(functools.partial(chunk_kernel, 0), both, out_rows)
    mixed = rows_out(total_kernel, mine, *arrived)
    log_sum = jnp.concatenate([outer_log[:WINDOW], inner_log, outer_log[WINDOW:]])
    return (mixed, log_sum.T)


def solution(mesh):
    torus = Mesh(mesh.devices.reshape(16, 4, 2, mesh.shape["tp"]), SP_TP)
    return jax.shard_map(
        layer,
        mesh=torus,
        in_specs=(
            P(SP, "tp"),
            P(),
            P(SP, "tp"),
            P(SP, "tp"),
            P(SP, "tp"),
            P(SP, "tp"),
            P(SP, "tp"),
            P(SP, "tp"),
            P(None, "tp"),
            P("tp"),
            P("tp", SP),
            P("tp", SP),
        ),
        out_specs=(P(SP_TP, None), P("tp", SP)),
        check_vma=False,
    )
```

```python
import jax
import jax.numpy as jnp
from jax import lax
from jax.experimental import pallas as pl
from jax.experimental.pallas import tpu as pltpu
from jax.sharding import Mesh
from jax.sharding import PartitionSpec as P


HEAD_DIM = 64
WINDOW = 128
GRID_W = 64
TOKENS = 65536
SP = ("sp_0", "sp_1", "sp_2")
SP_TP = (*SP, "tp")


rope_base = 10000.0
norm_eps = 1e-06


Z, X, CORE = "sp_0", "sp_1", "sp_2"
VMEM = pl.BlockSpec(memory_space=pltpu.VMEM)
SMEM = pl.BlockSpec(memory_space=pltpu.SMEM)


def params(mib):
    return pltpu.CompilerParams(vmem_limit_bytes=mib * 1024 * 1024)


def from_offset(x, axis, offset):
    count = lax.axis_size(axis)
    return lax.ppermute(x, axis, [((i + offset) % count, i) for i in range(count)])


def after(x, other):
    return lax.optimization_barrier((x, other))[0]


def gathered_parts(own):
    far = from_offset(own, X, 2)
    up, down = from_offset(own, X, 1), from_offset(own, X, 3)
    mine = (own, up, far, down)
    swapped = []
    for part in (own, up, far, down):
        swapped.append(from_offset(part, CORE, 1))
    return (*mine, *swapped)


def stage_kernel(tokens_ref, gain_ref, staged_tokens_ref, staged_gain_ref):
    staged_tokens_ref[...] = tokens_ref[...]
    staged_gain_ref[...] = gain_ref[...]


def staged(tokens, gain):
    return pl.pallas_call(
        stage_kernel,
        out_shape=(
            jax.ShapeDtypeStruct(tokens.shape, tokens.dtype),
            jax.ShapeDtypeStruct(gain.shape, gain.dtype),
        ),
        in_specs=[VMEM] * 2,
        out_specs=(VMEM,) * 2,
        compiler_params=params(4),
        cost_estimate=pl.CostEstimate(flops=500_000, bytes_accessed=1_000_000, transcendentals=0),
    )(tokens, gain)


def norm_kernel(gain_ref, *refs):
    tokens, normed_ref = refs[:4], refs[4]
    tp = lax.axis_index("tp")
    rows, width = tokens[0].shape
    step_rows = 64

    def norm_step(step, carry):
        at = pl.ds(pl.multiple_of(step * step_rows, step_rows), step_rows)
        blocks = [ref[at, :].astype(jnp.float32) for ref in tokens]
        square = sum(jnp.sum(b * b, axis=1, keepdims=True) for b in blocks)
        scale = lax.rsqrt(square / (4 * width) + norm_eps)
        for k, b in enumerate(blocks):
            cols = pl.ds(pl.multiple_of(lax.rem(tp + k, 4) * width, width), width)
            normed_ref[at, cols] = (b * scale * gain_ref[:, cols]).astype(jnp.bfloat16)
        return carry

    lax.fori_loop(0, rows // step_rows, norm_step, 0)


def normalized(gain, tokens):
    rows, width = tokens[0].shape
    return pl.pallas_call(
        norm_kernel,
        out_shape=jax.ShapeDtypeStruct((rows, 4 * width), jnp.bfloat16),
        in_specs=[VMEM] * 5,
        out_specs=VMEM,
        compiler_params=params(8),
        cost_estimate=pl.CostEstimate(
            flops=500_000_000, bytes_accessed=4_000_000, transcendentals=512
        ),
    )(gain, *tokens)


def place_rows(parts, out_ref, columns):
    x, core = lax.axis_index(X), lax.axis_index(CORE)
    for side in range(2):
        for x_rel in range(4):
            ref = parts[4 * side + x_rel]
            place = lax.rem(x + x_rel, 4) * 2 + lax.rem(core + side, 2)
            for z in range(16):
                at = pl.ds(pl.multiple_of(z * 128 + place * 16, 16), 16)
                out_ref[at, :] = ref[z, :, columns]


def rotated(x, cosine, sine):
    width = x.shape[-1]
    lane = lax.broadcasted_iota(jnp.int32, x.shape, 1)
    ahead = pltpu.roll(x, width - 16, 1)
    behind = pltpu.roll(x, 16, 1)
    return x * cosine + jnp.where(lane % 32 < 16, ahead, behind) * sine


def project_kernel(*refs):
    normed_ref, cos_ref, sin_ref = refs[:3]
    kvc_ref, query_ref, post_ref, out_rows_ref, rows_ref = refs[11:]
    place_rows(refs[3:11], rows_ref, slice(0, 1152))
    place_rows(refs[3:11], out_rows_ref, slice(1152, 1664))

    def projected(first, last):
        return jnp.dot(
            normed_ref[...], rows_ref[:, first:last], preferred_element_type=jnp.float32
        )

    key_value = projected(0, 128)
    lane = lax.broadcasted_iota(jnp.int32, key_value.shape, 1)
    cosine = cos_ref[...]
    sine = sin_ref[...]
    kvc_ref[:, :128] = jnp.where(
        lane < 64, rotated(key_value, cosine, sine), key_value
    ).astype(jnp.bfloat16)
    kvc_ref[:, 128:] = (projected(128, 384) * projected(384, 640)).astype(jnp.bfloat16)
    for half in range(2):
        part = projected(640 + 128 * half, 768 + 128 * half)
        query_ref[:, 128 * half : 128 * (half + 1)] = rotated(part, cosine, sine).astype(
            jnp.bfloat16
        )
    post_ref[...] = projected(896, 1152)


def project(normed, cosine, sine, parts):
    rows = normed.shape[0]
    return pl.pallas_call(
        project_kernel,
        out_shape=(
            jax.ShapeDtypeStruct((rows, 384), jnp.bfloat16),
            jax.ShapeDtypeStruct((rows, 256), jnp.bfloat16),
            jax.ShapeDtypeStruct((rows, 256), jnp.float32),
            jax.ShapeDtypeStruct((2048, 512), jnp.bfloat16),
        ),
        in_specs=[VMEM] * 11,
        out_specs=(VMEM,) * 4,
        scratch_shapes=[pltpu.VMEM((2048, 1152), jnp.bfloat16)],
        compiler_params=params(24),
        cost_estimate=pl.CostEstimate(
            flops=2 * rows * 2048 * 1152, bytes_accessed=8_000_000, transcendentals=0
        ),
    )(normed, cosine, sine, *parts)


def window_bias():
    row = lax.broadcasted_iota(jnp.int32, (WINDOW, 3 * WINDOW), 0)
    col = lax.broadcasted_iota(jnp.int32, (WINDOW, 3 * WINDOW), 1)
    return jnp.where((col >= row) & (col <= row + 2 * WINDOW), 0.0, -jnp.inf)


def inside_sequence(bias, first_key):
    key_pos = first_key + lax.broadcasted_iota(jnp.int32, bias.shape, 1)
    return jnp.where((key_pos >= 0) & (key_pos < TOKENS), bias, -jnp.inf)


def attended_block(query, keys, values, sinks, bias):
    heads = query.shape[1] // HEAD_DIM
    query = query * jnp.bfloat16(HEAD_DIM**-0.5)
    stacked = jnp.concatenate(
        [query[:, HEAD_DIM * h : HEAD_DIM * (h + 1)] for h in range(heads)], axis=0
    )
    scores = lax.dot_general(
        stacked, keys, (((1,), (1,)), ((), ())), preferred_element_type=jnp.float32
    )
    results, logs = [], []
    for h in range(heads):
        own = scores[WINDOW * h : WINDOW * (h + 1)] + bias
        row_max = jnp.maximum(jnp.max(own, axis=1, keepdims=True), sinks[h])
        exp_scores = jnp.exp(own - row_max)
        denominator = jnp.sum(exp_scores, axis=1, keepdims=True) + jnp.exp(sinks[h] - row_max)
        results.append((exp_scores * (1.0 / denominator)).astype(jnp.bfloat16))
        logs.append(row_max + jnp.log(denominator))
    weights = jnp.concatenate(results, axis=0)
    result = jnp.dot(weights, values, preferred_element_type=jnp.float32).astype(jnp.bfloat16)
    return (
        jnp.concatenate([result[WINDOW * h : WINDOW * (h + 1)] for h in range(heads)], axis=1),
        jnp.concatenate(logs, axis=1),
    )


def first_position():
    return lax.axis_index(SP) * 512


def inner_kernel(sink_ref, query_ref, kvc_ref, attended_ref, log_ref):
    sinks = [sink_ref[h] for h in range(4)]
    bias = window_bias()
    for n in (1, 2):
        window = slice((n - 1) * WINDOW, (n + 2) * WINDOW)
        result, log_sum = attended_block(
            query_ref[n * WINDOW : (n + 1) * WINDOW, :],
            kvc_ref[window, :HEAD_DIM],
            kvc_ref[window, HEAD_DIM : 2 * HEAD_DIM],
            sinks,
            bias,
        )
        attended_ref[(n - 1) * WINDOW : n * WINDOW, :] = result
        log_ref[(n - 1) * WINDOW : n * WINDOW, :] = log_sum


def inner(sinks, query, kvc):
    return pl.pallas_call(
        inner_kernel,
        out_shape=(
            jax.ShapeDtypeStruct((256, 256), jnp.bfloat16),
            jax.ShapeDtypeStruct((256, 4), jnp.float32),
        ),
        in_specs=[SMEM, VMEM, VMEM],
        out_specs=(VMEM, VMEM),
        compiler_params=params(12),
        cost_estimate=pl.CostEstimate(
            flops=2 * 2 * 1024 * 384 * 64 * 20, bytes_accessed=2_000_000, transcendentals=400_000
        ),
    )(sinks, query, kvc)


def outer_kernel(
    sink_ref, query_ref, kvc_ref, low_ref, high_ref, post_ref, taps_ref, inner_ref, out_rows_ref,
    *refs,
):
    far_ref, both_ref, log_ref = refs
    sinks = [sink_ref[h] for h in range(4)]
    offset = first_position()
    bias = window_bias()
    rows = query_ref.shape[0]
    edges = (
        (0, jnp.concatenate([low_ref[:, :128], kvc_ref[: 2 * WINDOW, :128]], axis=0)),
        (3, jnp.concatenate([kvc_ref[rows - 2 * WINDOW :, :128], high_ref[:, :128]], axis=0)),
    )
    for k, (n, window) in enumerate(edges):
        result, log_sum = attended_block(
            query_ref[n * WINDOW : (n + 1) * WINDOW, :],
            window[:, :HEAD_DIM],
            window[:, HEAD_DIM:],
            sinks,
            inside_sequence(bias, offset + (n - 1) * WINDOW),
        )
        both_ref[n * WINDOW : (n + 1) * WINDOW, :256] = result
        log_ref[k * WINDOW : (k + 1) * WINDOW, :] = log_sum
    both_ref[WINDOW : 3 * WINDOW, :256] = inner_ref[...]
    conv = kvc_ref[:, 128:].astype(jnp.float32)
    row = lax.broadcasted_iota(jnp.int32, conv.shape, 0)
    before = low_ref[WINDOW - 16 :, 128:].astype(jnp.float32)[15:16]
    after = high_ref[:16, 128:].astype(jnp.float32)[0:1]
    previous = jnp.where(row == 0, before, pltpu.roll(conv, 1, 0))
    following = jnp.where(row == rows - 1, after, pltpu.roll(conv, rows - 1, 0))
    convolved = taps_ref[0:1] * previous + taps_ref[1:2] * conv + taps_ref[2:3] * following
    both_ref[:, 256:] = (post_ref[...] * convolved).astype(jnp.bfloat16)
    far_ref[...] = chunk(both_ref, out_rows_ref, 2).astype(jnp.bfloat16)


def chunk(both_ref, out_rows_ref, step):
    block = lax.rem(lax.axis_index("tp") + step, 4)
    return lax.dot_general(
        both_ref[pl.ds(pl.multiple_of(block * WINDOW, WINDOW), WINDOW), :],
        out_rows_ref[...],
        (((1,), (1,)), ((), ())),
        preferred_element_type=jnp.float32,
    )


def near_kernel(both_ref, out_rows_ref, up_ref, down_ref):
    up_ref[...] = chunk(both_ref, out_rows_ref, 1).astype(jnp.bfloat16)
    down_ref[...] = chunk(both_ref, out_rows_ref, 3).astype(jnp.bfloat16)


def own_kernel(both_ref, out_rows_ref, own_ref):
    own_ref[...] = chunk(both_ref, out_rows_ref, 0).astype(jnp.bfloat16)


def chunks(kernel, count, *arrays):
    return pl.pallas_call(
        kernel,
        out_shape=(jax.ShapeDtypeStruct((128, 2048), jnp.bfloat16),) * count,
        in_specs=[VMEM] * len(arrays),
        out_specs=(VMEM,) * count,
        compiler_params=params(12),
        cost_estimate=pl.CostEstimate(
            flops=count * 2 * 128 * 512 * 2048, bytes_accessed=3_000_000, transcendentals=0
        ),
    )(*arrays)


def outer(sinks, query, kvc, low, high, post, taps, inner_attended, out_rows):
    return pl.pallas_call(
        outer_kernel,
        out_shape=(
            jax.ShapeDtypeStruct((128, 2048), jnp.bfloat16),
            jax.ShapeDtypeStruct((512, 512), jnp.bfloat16),
            jax.ShapeDtypeStruct((256, 4), jnp.float32),
        ),
        in_specs=[SMEM] + [VMEM] * 8,
        out_specs=(VMEM,) * 3,
        compiler_params=params(8),
        cost_estimate=pl.CostEstimate(
            flops=2 * 512 * 512 * 2048, bytes_accessed=8_000_000, transcendentals=400_000
        ),
    )(sinks, query, kvc, low, high, post, taps, inner_attended, out_rows)


def halo(block, width):
    count = lax.axis_size(SP)
    forward = [(i, i + 1) for i in range(count - 1)]
    backward = [(i + 1, i) for i in range(count - 1)]
    low = lax.ppermute(block[-width:], SP, forward)
    high = lax.ppermute(block[:width], SP, backward)
    return low, high


def rotation_tables(rows):
    shape = (rows, 2 * HEAD_DIM)
    lane = lax.broadcasted_iota(jnp.int32, shape, 1)
    position = lax.axis_index(SP) * rows + lax.broadcasted_iota(jnp.int32, shape, 0)
    half_dim = HEAD_DIM // 2
    inv_freq = rope_base ** (-(2 * (lane % 16)).astype(jnp.float32) / half_dim)
    index = jnp.where(lane % HEAD_DIM < half_dim, position // GRID_W, position % GRID_W)
    angle = index.astype(jnp.float32) * inv_freq
    sine = jnp.sin(angle)
    return jnp.cos(angle), jnp.where(lane % half_dim < 16, -sine, sine)


def layer(
    tokens,
    norm_gain,
    w_query,
    w_key,
    w_value,
    w_post_gate,
    w_pre_gate,
    w_conv_in,
    conv_taps,
    sink_logit,
    w_out_attn,
    w_out_conv,
):
    rows = tokens.shape[0]
    piece = jnp.concatenate(
        [
            w_key,
            w_value,
            w_pre_gate,
            w_conv_in,
            w_query,
            w_post_gate,
            w_out_attn.T,
            w_out_conv.T,
        ],
        axis=1,
    )
    cosine, sine = rotation_tables(rows)
    own = lax.all_gather(after(piece, (cosine, sine)), Z, axis=0)
    parts = gathered_parts(own)
    late_tokens = after(tokens, own)
    arrived = [from_offset(late_tokens, "tp", step) for step in (1, 2, 3)]
    own_tokens, gain = staged(tokens, norm_gain[None])
    normed = normalized(gain, [own_tokens, *arrived])
    kvc, query, post, out_rows = project(normed, cosine, sine, parts)
    low, high = halo(kvc, WINDOW)
    inner_attended, inner_log = inner(sink_logit, query, kvc)
    far, both, outer_log = outer(
        sink_logit, query, kvc, low, high, post, conv_taps, inner_attended, out_rows
    )
    arrived = [from_offset(far, "tp", -2)]
    up, down = chunks(near_kernel, 2, both, out_rows)
    arrived += [from_offset(up, "tp", -1), from_offset(down, "tp", 1)]
    (mine,) = chunks(own_kernel, 1, both, out_rows)
    total = mine.astype(jnp.float32)
    for block in arrived:
        total = total + block.astype(jnp.float32)
    log_sum = jnp.concatenate([outer_log[:WINDOW], inner_log, outer_log[WINDOW:]])
    return (total.astype(jnp.bfloat16), log_sum.T)


def solution(mesh):
    torus = Mesh(mesh.devices.reshape(16, 4, 2, mesh.shape["tp"]), SP_TP)
    return jax.shard_map(
        layer,
        mesh=torus,
        in_specs=(
            P(SP, "tp"),
            P(),
            P(SP, "tp"),
            P(SP, "tp"),
            P(SP, "tp"),
            P(SP, "tp"),
            P(SP, "tp"),
            P(SP, "tp"),
            P(None, "tp"),
            P("tp"),
            P("tp", SP),
            P("tp", SP),
        ),
        out_specs=(P(SP_TP, None), P("tp", SP)),
        check_vma=False,
    )
```

```python
import jax
import jax.numpy as jnp
import numpy as np
from jax import lax
from jax.experimental import pallas as pl
from jax.experimental.pallas import tpu as pltpu
from jax.sharding import Mesh
from jax.sharding import PartitionSpec as P


HEAD_DIM = 64
WINDOW = 128
GRID_W = 64
TOKENS = 65536
SP = ("sp_0", "sp_1", "sp_2")
SP_TP = (*SP, "tp")


rope_base = 10000.0
norm_eps = 1e-06


Z, X, CORE = "sp_0", "sp_1", "sp_2"
VMEM = pl.BlockSpec(memory_space=pltpu.VMEM)
SMEM = pl.BlockSpec(memory_space=pltpu.SMEM)


def params(mib):
    return pltpu.CompilerParams(vmem_limit_bytes=mib * 1024 * 1024)


def from_offset(x, axis, offset):
    count = lax.axis_size(axis)
    return lax.ppermute(x, axis, [((i + offset) % count, i) for i in range(count)])


def after(x, other):
    return lax.optimization_barrier((x, other))[0]


def gathered_parts(own):
    far = from_offset(own, X, 2)
    up = from_offset(own, X, 1)
    down = from_offset(own, X, 3)
    mine = (own, up, far, down)
    swapped = []
    for part in (own, up, far, down):
        swapped.append(from_offset(part, CORE, 1))
    return (*mine, *swapped)


def stage_kernel(
    tokens_ref, gain_ref, freq_ref, staged_tokens_ref, staged_gain_ref, cos_ref, sin_ref
):
    staged_tokens_ref[...] = tokens_ref[...]
    staged_gain_ref[...] = gain_ref[...]
    first = first_position()
    step_rows = 64

    def table_step(step, carry):
        start = pl.multiple_of(step * step_rows, step_rows)
        shape = (step_rows, cos_ref.shape[1])
        position = first + start + lax.broadcasted_iota(jnp.int32, shape, 0)
        lane = lax.broadcasted_iota(jnp.int32, shape, 1)
        index = jnp.where(lane % HEAD_DIM < HEAD_DIM // 2, position // GRID_W, position % GRID_W)
        angle = index.astype(jnp.float32) * freq_ref[...]
        sine = jnp.sin(angle)
        cos_ref[pl.ds(start, step_rows), :] = jnp.cos(angle)
        sin_ref[pl.ds(start, step_rows), :] = jnp.where(lane % 32 < 16, -sine, sine)
        return carry

    lax.fori_loop(0, cos_ref.shape[0] // step_rows, table_step, 0)


def staged(tokens, gain):
    half_dim = HEAD_DIM // 2
    lane = np.arange(2 * HEAD_DIM)
    exponent = -(2 * (lane % 16)).astype(np.float32) / np.float32(half_dim)
    inv_freq = (np.float32(rope_base) ** exponent).astype(np.float32)[None]
    table = jax.ShapeDtypeStruct((tokens.shape[0], 2 * HEAD_DIM), jnp.float32)
    return pl.pallas_call(
        stage_kernel,
        out_shape=(
            jax.ShapeDtypeStruct(tokens.shape, tokens.dtype),
            jax.ShapeDtypeStruct(gain.shape, gain.dtype),
            table,
            table,
        ),
        in_specs=[VMEM] * 3,
        out_specs=(VMEM,) * 4,
        compiler_params=params(6),
        cost_estimate=pl.CostEstimate(
            flops=20_000_000, bytes_accessed=2_000_000, transcendentals=131072
        ),
    )(tokens, gain, jnp.asarray(inv_freq))


def norm_kernel(gain_ref, *refs):
    tokens, normed_ref = refs[:4], refs[4]
    tp = lax.axis_index("tp")
    rows, width = tokens[0].shape
    step_rows = 64

    def norm_step(step, carry):
        at = pl.ds(pl.multiple_of(step * step_rows, step_rows), step_rows)
        blocks = [ref[at, :].astype(jnp.float32) for ref in tokens]
        square = sum(jnp.sum(b * b, axis=1, keepdims=True) for b in blocks)
        scale = lax.rsqrt(square / (4 * width) + norm_eps)
        for k, b in enumerate(blocks):
            cols = pl.ds(pl.multiple_of(lax.rem(tp + k, 4) * width, width), width)
            normed_ref[at, cols] = (b * scale * gain_ref[:, cols]).astype(jnp.bfloat16)
        return carry

    lax.fori_loop(0, rows // step_rows, norm_step, 0)


def normalized(gain, tokens):
    rows, width = tokens[0].shape
    return pl.pallas_call(
        norm_kernel,
        out_shape=jax.ShapeDtypeStruct((rows, 4 * width), jnp.bfloat16),
        in_specs=[VMEM] * 5,
        out_specs=VMEM,
        compiler_params=params(8),
        cost_estimate=pl.CostEstimate(
            flops=500_000_000, bytes_accessed=4_000_000, transcendentals=512
        ),
    )(gain, *tokens)


def place_rows(parts, out_ref, columns):
    x, core = lax.axis_index(X), lax.axis_index(CORE)
    for side in range(2):
        for x_rel in range(4):
            ref = parts[4 * side + x_rel]
            place = lax.rem(x + x_rel, 4) * 2 + lax.rem(core + side, 2)
            for z in range(16):
                at = pl.ds(pl.multiple_of(z * 128 + place * 16, 16), 16)
                out_ref[at, :] = ref[z, :, columns]


def rotated(x, cosine, sine):
    width = x.shape[-1]
    lane = lax.broadcasted_iota(jnp.int32, x.shape, 1)
    ahead = pltpu.roll(x, width - 16, 1)
    behind = pltpu.roll(x, 16, 1)
    return x * cosine + jnp.where(lane % 32 < 16, ahead, behind) * sine


def project_kernel(*refs):
    normed_ref, cos_ref, sin_ref = refs[:3]
    kvc_ref, query_ref, post_ref, out_rows_ref, rows_ref = refs[11:]
    place_rows(refs[3:11], rows_ref, slice(0, 1152))
    place_rows(refs[3:11], out_rows_ref, slice(1152, 1664))

    def projected(first, last):
        return jnp.dot(
            normed_ref[...], rows_ref[:, first:last], preferred_element_type=jnp.float32
        )

    key_value = projected(0, 128)
    lane = lax.broadcasted_iota(jnp.int32, key_value.shape, 1)
    cosine = cos_ref[...]
    sine = sin_ref[...]
    kvc_ref[:, :128] = jnp.where(
        lane < 64, rotated(key_value, cosine, sine), key_value
    ).astype(jnp.bfloat16)
    kvc_ref[:, 128:] = (projected(128, 384) * projected(384, 640)).astype(jnp.bfloat16)
    for half in range(2):
        part = projected(640 + 128 * half, 768 + 128 * half)
        query_ref[:, 128 * half : 128 * (half + 1)] = rotated(part, cosine, sine).astype(
            jnp.bfloat16
        )
    post_ref[...] = projected(896, 1152)


def project(normed, cosine, sine, parts):
    rows = normed.shape[0]
    return pl.pallas_call(
        project_kernel,
        out_shape=(
            jax.ShapeDtypeStruct((rows, 384), jnp.bfloat16),
            jax.ShapeDtypeStruct((rows, 256), jnp.bfloat16),
            jax.ShapeDtypeStruct((rows, 256), jnp.float32),
            jax.ShapeDtypeStruct((2048, 512), jnp.bfloat16),
        ),
        in_specs=[VMEM] * 11,
        out_specs=(VMEM,) * 4,
        scratch_shapes=[pltpu.VMEM((2048, 1152), jnp.bfloat16)],
        compiler_params=params(24),
        cost_estimate=pl.CostEstimate(
            flops=2 * rows * 2048 * 1152, bytes_accessed=8_000_000, transcendentals=0
        ),
    )(normed, cosine, sine, *parts)


def window_bias():
    row = lax.broadcasted_iota(jnp.int32, (WINDOW, 3 * WINDOW), 0)
    col = lax.broadcasted_iota(jnp.int32, (WINDOW, 3 * WINDOW), 1)
    return jnp.where((col >= row) & (col <= row + 2 * WINDOW), 0.0, -jnp.inf)


def inside_sequence(bias, first_key):
    key_pos = first_key + lax.broadcasted_iota(jnp.int32, bias.shape, 1)
    return jnp.where((key_pos >= 0) & (key_pos < TOKENS), bias, -jnp.inf)


def attended_block(query, keys, values, sinks, bias):
    heads = query.shape[1] // HEAD_DIM
    query = query * jnp.bfloat16(HEAD_DIM**-0.5)
    stacked = jnp.concatenate(
        [query[:, HEAD_DIM * h : HEAD_DIM * (h + 1)] for h in range(heads)], axis=0
    )
    scores = lax.dot_general(
        stacked, keys, (((1,), (1,)), ((), ())), preferred_element_type=jnp.float32
    )
    results, logs = [], []
    for h in range(heads):
        own = scores[WINDOW * h : WINDOW * (h + 1)] + bias
        row_max = jnp.maximum(jnp.max(own, axis=1, keepdims=True), sinks[h])
        exp_scores = jnp.exp(own - row_max)
        denominator = jnp.sum(exp_scores, axis=1, keepdims=True) + jnp.exp(sinks[h] - row_max)
        results.append((exp_scores * (1.0 / denominator)).astype(jnp.bfloat16))
        logs.append(row_max + jnp.log(denominator))
    weights = jnp.concatenate(results, axis=0)
    result = jnp.dot(weights, values, preferred_element_type=jnp.float32).astype(jnp.bfloat16)
    return (
        jnp.concatenate([result[WINDOW * h : WINDOW * (h + 1)] for h in range(heads)], axis=1),
        jnp.concatenate(logs, axis=1),
    )


def first_position():
    return lax.axis_index(SP) * 512


def inner_kernel(sink_ref, query_ref, kvc_ref, attended_ref, log_ref):
    sinks = [sink_ref[h] for h in range(4)]
    bias = window_bias()
    for n in (1, 2):
        window = slice((n - 1) * WINDOW, (n + 2) * WINDOW)
        result, log_sum = attended_block(
            query_ref[n * WINDOW : (n + 1) * WINDOW, :],
            kvc_ref[window, :HEAD_DIM],
            kvc_ref[window, HEAD_DIM : 2 * HEAD_DIM],
            sinks,
            bias,
        )
        attended_ref[(n - 1) * WINDOW : n * WINDOW, :] = result
        log_ref[(n - 1) * WINDOW : n * WINDOW, :] = log_sum


def inner(sinks, query, kvc):
    return pl.pallas_call(
        inner_kernel,
        out_shape=(
            jax.ShapeDtypeStruct((256, 256), jnp.bfloat16),
            jax.ShapeDtypeStruct((256, 4), jnp.float32),
        ),
        in_specs=[SMEM, VMEM, VMEM],
        out_specs=(VMEM, VMEM),
        compiler_params=params(12),
        cost_estimate=pl.CostEstimate(
            flops=2 * 2 * 1024 * 384 * 64 * 20, bytes_accessed=2_000_000, transcendentals=400_000
        ),
    )(sinks, query, kvc)


def outer_kernel(
    sink_ref, query_ref, kvc_ref, low_ref, high_ref, post_ref, taps_ref, inner_ref, out_rows_ref,
    *refs,
):
    far_ref, both_ref, log_ref = refs
    sinks = [sink_ref[h] for h in range(4)]
    offset = first_position()
    bias = window_bias()
    rows = query_ref.shape[0]
    edges = (
        (0, jnp.concatenate([low_ref[:, :128], kvc_ref[: 2 * WINDOW, :128]], axis=0)),
        (3, jnp.concatenate([kvc_ref[rows - 2 * WINDOW :, :128], high_ref[:, :128]], axis=0)),
    )
    for k, (n, window) in enumerate(edges):
        result, log_sum = attended_block(
            query_ref[n * WINDOW : (n + 1) * WINDOW, :],
            window[:, :HEAD_DIM],
            window[:, HEAD_DIM:],
            sinks,
            inside_sequence(bias, offset + (n - 1) * WINDOW),
        )
        both_ref[n * WINDOW : (n + 1) * WINDOW, :256] = result
        log_ref[k * WINDOW : (k + 1) * WINDOW, :] = log_sum
    both_ref[WINDOW : 3 * WINDOW, :256] = inner_ref[...]
    conv = kvc_ref[:, 128:].astype(jnp.float32)
    row = lax.broadcasted_iota(jnp.int32, conv.shape, 0)
    before = low_ref[WINDOW - 16 :, 128:].astype(jnp.float32)[15:16]
    after = high_ref[:16, 128:].astype(jnp.float32)[0:1]
    previous = jnp.where(row == 0, before, pltpu.roll(conv, 1, 0))
    following = jnp.where(row == rows - 1, after, pltpu.roll(conv, rows - 1, 0))
    convolved = taps_ref[0:1] * previous + taps_ref[1:2] * conv + taps_ref[2:3] * following
    both_ref[:, 256:] = (post_ref[...] * convolved).astype(jnp.bfloat16)
    far_ref[...] = chunk(both_ref, out_rows_ref, 2).astype(jnp.bfloat16)


def chunk(both_ref, out_rows_ref, step):
    block = lax.rem(lax.axis_index("tp") + step, 4)
    return lax.dot_general(
        both_ref[pl.ds(pl.multiple_of(block * WINDOW, WINDOW), WINDOW), :],
        out_rows_ref[...],
        (((1,), (1,)), ((), ())),
        preferred_element_type=jnp.float32,
    )


def near_kernel(both_ref, out_rows_ref, up_ref, down_ref):
    up_ref[...] = chunk(both_ref, out_rows_ref, 1).astype(jnp.bfloat16)
    down_ref[...] = chunk(both_ref, out_rows_ref, 3).astype(jnp.bfloat16)


def own_kernel(both_ref, out_rows_ref, own_ref):
    own_ref[...] = chunk(both_ref, out_rows_ref, 0).astype(jnp.bfloat16)


def chunks(kernel, count, *arrays):
    return pl.pallas_call(
        kernel,
        out_shape=(jax.ShapeDtypeStruct((128, 2048), jnp.bfloat16),) * count,
        in_specs=[VMEM] * len(arrays),
        out_specs=(VMEM,) * count,
        compiler_params=params(12),
        cost_estimate=pl.CostEstimate(
            flops=count * 2 * 128 * 512 * 2048, bytes_accessed=3_000_000, transcendentals=0
        ),
    )(*arrays)


def outer(sinks, query, kvc, low, high, post, taps, inner_attended, out_rows):
    return pl.pallas_call(
        outer_kernel,
        out_shape=(
            jax.ShapeDtypeStruct((128, 2048), jnp.bfloat16),
            jax.ShapeDtypeStruct((512, 512), jnp.bfloat16),
            jax.ShapeDtypeStruct((256, 4), jnp.float32),
        ),
        in_specs=[SMEM] + [VMEM] * 8,
        out_specs=(VMEM,) * 3,
        compiler_params=params(8),
        cost_estimate=pl.CostEstimate(
            flops=2 * 512 * 512 * 2048, bytes_accessed=8_000_000, transcendentals=400_000
        ),
    )(sinks, query, kvc, low, high, post, taps, inner_attended, out_rows)


def halo(block, width):
    count = lax.axis_size(SP)
    forward = [(i, i + 1) for i in range(count - 1)]
    backward = [(i + 1, i) for i in range(count - 1)]
    low = lax.ppermute(block[-width:], SP, forward)
    high = lax.ppermute(block[:width], SP, backward)
    return low, high


def layer(
    tokens,
    norm_gain,
    w_query,
    w_key,
    w_value,
    w_post_gate,
    w_pre_gate,
    w_conv_in,
    conv_taps,
    sink_logit,
    w_out_attn,
    w_out_conv,
):
    piece = jnp.concatenate(
        [
            w_key,
            w_value,
            w_pre_gate,
            w_conv_in,
            w_query,
            w_post_gate,
            w_out_attn.T,
            w_out_conv.T,
        ],
        axis=1,
    )
    own = lax.all_gather(piece, Z, axis=0)
    parts = gathered_parts(own)
    late_tokens = after(tokens, own)
    arrived = [from_offset(late_tokens, "tp", step) for step in (1, 2, 3)]
    own_tokens, gain, cosine, sine = staged(tokens, norm_gain[None])
    normed = normalized(gain, [own_tokens, *arrived])
    kvc, query, post, out_rows = project(normed, cosine, sine, parts)
    low, high = halo(kvc, WINDOW)
    inner_attended, inner_log = inner(sink_logit, query, kvc)
    far, both, outer_log = outer(
        sink_logit, query, kvc, low, high, post, conv_taps, inner_attended, out_rows
    )
    arrived = [from_offset(far, "tp", -2)]
    up, down = chunks(near_kernel, 2, both, out_rows)
    arrived += [from_offset(up, "tp", -1), from_offset(down, "tp", 1)]
    (mine,) = chunks(own_kernel, 1, both, out_rows)
    total = mine.astype(jnp.float32)
    for block in arrived:
        total = total + block.astype(jnp.float32)
    log_sum = jnp.concatenate([outer_log[:WINDOW], inner_log, outer_log[WINDOW:]])
    return (total.astype(jnp.bfloat16), log_sum.T)


def solution(mesh):
    torus = Mesh(mesh.devices.reshape(16, 4, 2, mesh.shape["tp"]), SP_TP)
    return jax.shard_map(
        layer,
        mesh=torus,
        in_specs=(
            P(SP, "tp"),
            P(),
            P(SP, "tp"),
            P(SP, "tp"),
            P(SP, "tp"),
            P(SP, "tp"),
            P(SP, "tp"),
            P(SP, "tp"),
            P(None, "tp"),
            P("tp"),
            P("tp", SP),
            P("tp", SP),
        ),
        out_specs=(P(SP_TP, None), P("tp", SP)),
        check_vma=False,
    )
```
